32 devices in a mesh: sp: 8 (over z, y), tp: 4 (over x, core).
Axes of the slice: x: 2, y: 2, z: 4, core: 2. Of those that a mesh axis runs over, the one named last changes fastest.
Arguments:
- mixer_input: bfloat16 [1024, 1024], P('sp', 'tp'), may hold values from -1800 to 1800
- time_step: float32 [2, 64], P(None, 'tp'), may hold values from 0 to 2, as said below
- damping: float32 [2, 1024, 64], P(None, 'sp', 'tp'), may hold values from 0 to 2
- input_map: bfloat16 [2, 2, 64, 64, 16], P(None, None, 'tp'), may hold values from -1 to 1
- readout: float32 [2, 2, 64, 16, 64], P(None, None, 'tp'), may hold values from -0.5 to 0.5
- skip_gain: float32 [1024], P('tp'), may hold values from -4 to 4
- out_gain: float32 [1024], P('tp'), may hold values from 0.1 to 1.9
- out_weight: bfloat16 [1024, 2048], replicated, may hold values from -0.1875 to 0.1875
- residual: bfloat16 [1024, 2048], P(('sp', 'tp')), may hold values from -6 to 6
- channel_gain: float32 [2048], replicated, may hold values from 0.1 to 1.9
- value_weight: bfloat16 [2048, 6144], P('sp', 'tp'), may hold values from -0.125 to 0.125
- gate_weight: bfloat16 [2048, 6144], P('sp', 'tp'), may hold values from -0.125 to 0.125
- value_taps: float32 [3, 6144], P(None, 'tp'), may hold values from -3 to 3
- gate_taps: float32 [3, 6144], P(None, 'tp'), may hold values from -3 to 3
- down_weight: bfloat16 [6144, 2048], P('tp', 'sp'), may hold values from -0.078125 to 0.078125
Outputs:
- output: bfloat16 [1024, 2048], P(('sp', 'tp'))
The draws below stay inside these ranges and needn't reach their ends.
Inputs may be any that keep to these rules, and one draw needn't show every extreme that they name: `time_step`: positive.
All inputs are finite; a program needn't handle non-finite values.
Results may differ from the reference program's by a relative error of at most 0.017.
Values may be sent and summed in bfloat16 or wider, within the bound.
A program may use at most 128 MiB of HBM per device.

```python
import math
import jax
import jax.numpy as jnp
from jax import lax

D = 2048
DS = 1024
GROUP = 16
STATE = 64
FF = 6144
TOK_DEV = 128
G = 64
TOKEN_POSITIONS = 1024
N_TP = 4


def draw_mixer_input(key, part):
    split_random_keys = jax.random.split(key, 3)
    column_pos = jnp.arange(DS, dtype=jnp.float32) / DS
    spread = math.log(10.0)
    noise = jnp.clip(jax.random.normal(split_random_keys[0], (TOKEN_POSITIONS, DS), jnp.float32), -5.0, 5.0)
    row_scale = jnp.exp(jax.random.uniform(split_random_keys[2], (TOKEN_POSITIONS, 1), jnp.float32, 0.0, spread))
    column_scale = jnp.exp(spread * column_pos)[None, :]
    return (noise * row_scale * column_scale).astype(jnp.float32).astype(jnp.bfloat16)


def draw_time_step(key, part):
    split_random_keys = jax.random.split(key, 3)
    group_count = DS // GROUP
    chance = jax.random.randint(split_random_keys[0], (2, group_count), 0, 16)
    quick = chance < 8
    quick_rate = jnp.exp(jax.random.uniform(split_random_keys[1], (2, group_count), jnp.float32, math.log(5.0 / TOK_DEV), math.log(16.0 / TOK_DEV)))
    slow_rate = jnp.exp(jax.random.uniform(split_random_keys[2], (2, group_count), jnp.float32, math.log(0.2 / TOKEN_POSITIONS), math.log(1.0 / TOKEN_POSITIONS)))
    return 2.0 * jnp.where(quick, quick_rate, slow_rate)


def draw_damping(key, part):
    split_random_keys = jax.random.split(key, 4)
    group_count = DS // GROUP
    blocks = TOKEN_POSITIONS // TOK_DEV
    baseline_rate = jnp.exp(jax.random.uniform(split_random_keys[0], (2, 1, group_count), jnp.float32, math.log(0.1), math.log(0.4))) / TOKEN_POSITIONS
    multiplier = jnp.exp(jax.random.uniform(split_random_keys[1], (2, blocks, group_count), jnp.float32, 0.0, math.log(4.0)))
    multiplier = jnp.repeat(multiplier, TOK_DEV, axis=1)
    spike_locations = jax.random.randint(split_random_keys[2], (2, 1, group_count, 3), 0, TOKEN_POSITIONS)
    dropped_fraction = jax.random.uniform(split_random_keys[3], (2, 1, group_count, 3), jnp.float32, 0.2, 0.33)
    token_position = jnp.arange(TOKEN_POSITIONS, dtype=jnp.int32)[None, :, None, None]
    sudden_spike = jnp.sum(jnp.where(token_position == spike_locations, -jnp.log1p(-dropped_fraction), 0.0), axis=3)
    return (baseline_rate * multiplier + sudden_spike).astype(jnp.float32)


def block_levels(rng, dims, cuts, smallest, top_value):
    level, own = 1.0, jax.random.fold_in(rng, 6)
    for axis_at, shards_of in cuts:
        draws = jnp.exp(jax.random.uniform(jax.random.fold_in(own, axis_at), (shards_of,), jnp.float32, smallest / len(cuts), top_value / len(cuts)))
        level = level * jnp.repeat(draws, dims[axis_at] // shards_of).reshape([-1 if axis == axis_at else 1 for axis in range(len(dims))])
    return level


def normal_values(rng, extent, scale, limit, cuts=(), kind=jnp.bfloat16):
    level = block_levels(rng, extent, cuts, -0.22, 0.18) if cuts else 1.0
    array = jax.random.normal(rng, extent, jnp.float32) * scale * level
    return jnp.minimum(jnp.maximum(array, -limit), limit).astype(kind)


def setup_inputs(seed: int = 0) -> dict:
    key_of = jax.random.split(jax.random.key(seed), 16)
    mixer_input = draw_mixer_input(jax.random.fold_in(key_of[15], 71), 0)
    time_step = draw_time_step(jax.random.fold_in(key_of[15], 71), 0)
    damping = draw_damping(jax.random.fold_in(key_of[15], 71), 0)
    input_map = normal_values(key_of[3], (2, 2, G, STATE, GROUP), (2 * GROUP) ** -0.5, 1.0, ((2, 4),))
    readout = normal_values(key_of[4], (2, 2, G, GROUP, STATE), (2 * STATE) ** -0.5, 0.5, ((2, 4),), jnp.float32)
    skip_gain = normal_values(key_of[5], (DS,), 1.0, 4.0, ((0, 4),), jnp.float32)
    out_gain = jnp.clip(1.0 + 0.18 * jax.random.normal(key_of[6], (DS,), jnp.float32), 0.1, 1.9)
    out_weight = normal_values(key_of[7], (DS, D), DS ** -0.5, 0.1875)
    residual = normal_values(key_of[8], (TOKEN_POSITIONS, D), 1.0, 6.0, ((0, 32),))
    channel_gain = jnp.clip(1.0 + 0.18 * jax.random.normal(key_of[9], (D,), jnp.float32), 0.1, 1.9)
    value_weight = normal_values(key_of[10], (D, FF), D ** -0.5, 0.125, ((0, 8), (1, 4)))
    gate_weight = normal_values(key_of[11], (D, FF), D ** -0.5, 0.125, ((0, 8), (1, 4)))
    value_taps = normal_values(key_of[12], (3, FF), 0.577, 3.0, ((1, 4),), jnp.float32)
    gate_taps = normal_values(key_of[13], (3, FF), 0.577, 3.0, ((1, 4),), jnp.float32)
    down_weight = normal_values(key_of[14], (FF, D), FF ** -0.5, 0.078125, ((0, 4), (1, 8)))
    return dict(mixer_input=mixer_input, time_step=time_step, damping=damping, input_map=input_map, readout=readout, skip_gain=skip_gain, out_gain=out_gain, out_weight=out_weight, residual=residual, channel_gain=channel_gain, value_weight=value_weight, gate_weight=gate_weight, value_taps=value_taps, gate_taps=gate_taps, down_weight=down_weight)


norm_eps = 1e-06
highest = lax.Precision.HIGHEST

def combine(earlier, latter):
    prod_real = latter[0] * earlier[0] - latter[1] * earlier[1]
    prod_imag = latter[0] * earlier[1] + latter[1] * earlier[0]
    sum_real = latter[0] * earlier[2] - latter[1] * earlier[3] + latter[2]
    sum_imag = latter[0] * earlier[3] + latter[1] * earlier[2] + latter[3]
    return (prod_real, prod_imag, sum_real, sum_imag)

def group_mixer(operands):
    group_input, step_pair, damp_pair, in_maps, out_maps = operands
    states = in_maps.shape[2]
    frequency = math.pi * jnp.arange(states, dtype=jnp.float32)
    result = jnp.zeros(group_input.shape, jnp.float32)
    for direction in range(2):
        step_size = step_pair[direction]
        rotation = step_size * frequency
        magnitude = jnp.exp(-0.5 * step_size - damp_pair[direction])[:, None]
        decay_real = magnitude * jnp.cos(rotation)[None, :]
        decay_imag = magnitude * jnp.sin(rotation)[None, :]
        in_scale = jnp.sqrt(-jnp.expm1(-step_size))
        drive_real = jnp.dot(group_input, in_maps[direction, 0].T, preferred_element_type=jnp.float32) * in_scale
        drive_imag = jnp.dot(group_input, in_maps[direction, 1].T, preferred_element_type=jnp.float32) * in_scale
        scanned = lax.associative_scan(combine, (decay_real, decay_imag, drive_real, drive_imag), reverse=direction == 1, axis=0)
        result = result + jnp.dot(scanned[2], out_maps[direction, 0].T, precision=highest)
        result = result - jnp.dot(scanned[3], out_maps[direction, 1].T, precision=highest)
    return result

def shifted_sum(values, tap_rows):
    widened = jnp.pad(values.astype(jnp.float32), ((1, 1), (0, 0)))
    return tap_rows[0] * widened[:-2] + tap_rows[1] * widened[1:-1] + tap_rows[2] * widened[2:]

def reference(mixer_input, time_step, damping, input_map, readout, skip_gain, out_gain, out_weight, residual, channel_gain, value_weight, gate_weight, value_taps, gate_taps, down_weight):
    tokens, channels = mixer_input.shape
    group_count = time_step.shape[1]
    group_width = channels // group_count
    grouped = jnp.transpose(mixer_input.reshape(tokens, group_count, group_width), (1, 0, 2))
    per_group = lax.map(group_mixer, (grouped, time_step.T, jnp.transpose(damping, (2, 0, 1)), jnp.moveaxis(input_map, 2, 0), jnp.moveaxis(readout, 2, 0)))
    mixed_y = jnp.transpose(per_group, (1, 0, 2)).reshape(tokens, channels) + skip_gain[None, :] * mixer_input.astype(jnp.float32)
    inverse = lax.rsqrt(lax.optimization_barrier(jnp.mean(mixed_y * mixed_y, axis=1, keepdims=True)) + norm_eps)
    normed_mix = (mixed_y * inverse * out_gain[None, :]).astype(jnp.bfloat16)
    mixed_rows = jnp.dot(normed_mix, out_weight, preferred_element_type=jnp.float32)
    hidden_state = (residual.astype(jnp.float32) + mixed_rows).astype(jnp.bfloat16)
    state_wide = hidden_state.astype(jnp.float32)
    scale_rows = lax.rsqrt(lax.optimization_barrier(jnp.mean(state_wide * state_wide, axis=1, keepdims=True)) + norm_eps)
    normed = (state_wide * scale_rows * channel_gain[None, :]).astype(jnp.bfloat16)
    value_up = jnp.dot(normed, value_weight, preferred_element_type=jnp.float32).astype(jnp.bfloat16)
    gate_up = jnp.dot(normed, gate_weight, preferred_element_type=jnp.float32).astype(jnp.bfloat16)
    value_conv = shifted_sum(value_up, value_taps)
    gate_conv = shifted_sum(gate_up, gate_taps)
    hidden = (value_conv * jax.nn.silu(gate_conv)).astype(jnp.bfloat16)
    block_width = FF // N_TP
    summed = jnp.zeros((tokens, out_weight.shape[1]), jnp.float32)
    for part_index in range(N_TP):
        first_col = part_index * block_width
        partial_value = jnp.dot(hidden[:, first_col:first_col + block_width], down_weight[first_col:first_col + block_width], preferred_element_type=jnp.float32)
        rounded = lax.optimization_barrier(partial_value.astype(jnp.bfloat16))
        summed = summed + rounded.astype(jnp.float32)
    return (state_wide + summed).astype(jnp.bfloat16)
```

```python
import math

import jax
import jax.numpy as jnp
from jax import lax
from jax.experimental import pallas as pl
from jax.experimental.pallas import tpu as pltpu
from jax.sharding import PartitionSpec as P

norm_eps = 1e-06
highest = lax.Precision.HIGHEST
mesh_ids = pl.DeviceIdType.MESH


def carry_kernel(count, own_ref, all_ref, local_sem, send_sem, recv_sem):
    sp, tp = lax.axis_index("sp"), lax.axis_index("tp")
    barrier = pltpu.get_barrier_semaphore()
    for offset in range(1, count):
        peer = lax.rem(sp + offset, count)
        pl.semaphore_signal(barrier, inc=1, device_id=(peer, tp), device_id_type=mesh_ids)
    pl.semaphore_wait(barrier, count - 1)
    keep = pltpu.make_async_copy(own_ref, all_ref.at[sp], local_sem)
    keep.start()
    copies = []
    for offset in range(1, count):
        peer = lax.rem(sp + offset, count)
        copy = pltpu.make_async_remote_copy(
            src_ref=own_ref,
            dst_ref=all_ref.at[sp],
            send_sem=send_sem.at[offset],
            recv_sem=recv_sem.at[offset],
            device_id=(peer, tp),
            device_id_type=mesh_ids,
        )
        copy.start()
        copies.append(copy)
    keep.wait()
    for copy in copies:
        copy.wait()


def gather_ends(packed, count):
    vmem = pl.BlockSpec(memory_space=pltpu.VMEM)
    return pl.pallas_call(
        lambda *refs: carry_kernel(count, *refs),
        name="gather_ends",
        out_shape=jax.ShapeDtypeStruct((count,) + packed.shape, packed.dtype),
        in_specs=[vmem],
        out_specs=vmem,
        scratch_shapes=[
            pltpu.SemaphoreType.DMA,
            pltpu.SemaphoreType.DMA((count,)),
            pltpu.SemaphoreType.DMA((count,)),
        ],
        compiler_params=pltpu.CompilerParams(collective_id=0, has_side_effects=True),
    )(packed)


gather_orders = (("z", "y", "x", "c"), ("y", "z", "x", "c"))
sum_orders = (("c", "x", "y", "z"), ("c", "z", "y", "x"))
axes = ("z", "y", "x", "c")


def channel_kernel(sizes, *refs):
    normed_ref, hidden_state_ref, up_send, down_send, taps_ref, out_ref = refs[:6]
    rows_all, up_rows, partial, up_land, down_land, down_ref = refs[6:12]
    landing = refs[12:20]
    local_sem, send_sem, recv_sem, weight_send_sem, weight_recv_sem = refs[20:25]
    rows, width = normed_ref.shape
    half = width // 2
    count, part, part_width = down_send.shape
    sp, tp = lax.axis_index("sp"), lax.axis_index("tp")
    mine = {
        "z": sp // sizes["y"],
        "y": lax.rem(sp, sizes["y"]),
        "x": tp // sizes["c"],
        "c": lax.rem(tp, sizes["c"]),
    }

    def neighbour(axis, offset):
        at = dict(mine)
        at[axis] = lax.rem(mine[axis] + offset, sizes[axis])
        return at[axis], (at["z"] * sizes["y"] + at["y"], at["x"] * sizes["c"] + at["c"])

    barrier = pltpu.get_barrier_semaphore()
    greeted = 0
    for axis in ("x", "c"):
        for offset in range(1, sizes[axis]):
            _, device = neighbour(axis, offset)
            pl.semaphore_signal(barrier, inc=1, device_id=device, device_id_type=mesh_ids)
            greeted += 1
    for offset in range(1, count):
        peer = lax.rem(sp + offset, count)
        pl.semaphore_signal(barrier, inc=1, device_id=(peer, tp), device_id_type=mesh_ids)
        greeted += 1
    pl.semaphore_wait(barrier, greeted)

    keeps = []
    for kind, (source, target) in enumerate(
        (
            (normed_ref, rows_all.at[mine["z"], mine["y"], mine["x"], mine["c"]]),
            (up_send.at[sp], up_land.at[sp]),
            (down_send.at[sp], down_land.at[sp]),
        )
    ):
        keep = pltpu.make_async_copy(source, target, local_sem.at[kind])
        keep.start()
        keeps.append(keep)
    keeps[0].wait()

    def spread(source, land, kind):
        started = []
        for offset in range(1, count):
            peer = lax.rem(sp + offset, count)
            copy = pltpu.make_async_remote_copy(
                src_ref=source.at[peer],
                dst_ref=land.at[sp],
                send_sem=weight_send_sem.at[kind, offset],
                recv_sem=weight_recv_sem.at[kind, offset],
                device_id=(peer, tp),
                device_id_type=mesh_ids,
            )
            copy.start()
            started.append(copy)
        return started

    slot = 0
    pending = [[], []]
    up_copies, down_copies = [], []
    for stage in range(4):
        if stage == 2:
            up_copies = spread(up_send, up_land, 0)
            down_copies = spread(down_send, down_land, 1)
        for piece in range(2):
            axis = gather_orders[piece][stage]
            done = gather_orders[piece][:stage]
            for copy in pending[piece]:
                copy.wait()
            pending[piece] = []
            index = tuple(slice(None) if name in done else mine[name] for name in axes)
            block = rows_all.at[index + (slice(None), pl.ds(piece * half, half))]
            for offset in range(1, sizes[axis]):
                _, device = neighbour(axis, offset)
                copy = pltpu.make_async_remote_copy(
                    src_ref=block,
                    dst_ref=block,
                    send_sem=send_sem.at[slot],
                    recv_sem=recv_sem.at[slot],
                    device_id=device,
                    device_id_type=mesh_ids,
                )
                copy.start()
                pending[piece].append(copy)
                slot += 1
    for piece in range(2):
        for copy in pending[piece]:
            copy.wait()

    plane = sizes["y"] * sizes["x"] * sizes["c"] * rows
    total = plane * sizes["z"]
    for copy in [keeps[1]] + up_copies:
        copy.wait()
    edge = jnp.zeros((8, up_rows.shape[1]), jnp.float32)
    up_rows[pl.ds(0, 8), :] = edge
    up_rows[pl.ds(total + 8, 8), :] = edge

    def project(z, _):
        block = rows_all[z].reshape(plane, width)
        up_weight = up_land[...].reshape(width, 2 * part)
        up = jnp.dot(block, up_weight, preferred_element_type=jnp.float32)
        start = pl.multiple_of(z * plane + 8, 8)
        up_rows[pl.ds(start, plane), :] = up.astype(jnp.bfloat16).astype(jnp.float32)
        return _

    lax.fori_loop(0, sizes["z"], project, 0)

    for copy in [keeps[2]] + down_copies:
        copy.wait()
    for source in range(count):
        down_ref[:, source * part_width : (source + 1) * part_width] = down_land[source]

    def mix(z, _):
        start = pl.multiple_of(z * plane, 8)
        window = up_rows[pl.ds(start, plane + 16), :]
        convolved = (
            taps_ref[0:1, :] * window[7 : plane + 7]
            + taps_ref[1:2, :] * window[8 : plane + 8]
            + taps_ref[2:3, :] * window[9 : plane + 9]
        )
        gate = convolved[:, part:]
        hidden = convolved[:, :part] * (gate / (1.0 + jnp.exp(-gate)))
        sums = jnp.dot(
            hidden.astype(jnp.bfloat16), down_ref[...], preferred_element_type=jnp.float32
        )
        partial[z] = sums.astype(jnp.bfloat16).reshape(partial.shape[1:])
        return _

    lax.fori_loop(0, sizes["z"], mix, 0)

    def start_sum(piece, stage, slot):
        axis = sum_orders[piece][stage]
        done = sum_orders[piece][:stage]
        started = []
        for offset in range(1, sizes[axis]):
            place, device = neighbour(axis, offset)
            index = tuple(
                place if name == axis else mine[name] if name in done else slice(None)
                for name in axes
            )
            copy = pltpu.make_async_remote_copy(
                src_ref=partial.at[index + (slice(None), pl.ds(piece * half, half))],
                dst_ref=landing[piece * 4 + stage].at[offset - 1],
                send_sem=send_sem.at[slot],
                recv_sem=recv_sem.at[slot],
                device_id=device,
                device_id_type=mesh_ids,
            )
            copy.start()
            started.append(copy)
            slot += 1
        return started, slot

    def add_landed(piece, stage):
        axis = sum_orders[piece][stage]
        done = sum_orders[piece][: stage + 1]
        land = landing[piece * 4 + stage]
        columns = pl.ds(piece * half, half)
        free = [name for name in axes if name not in done]

        def add(step, _):
            index, inner = [], ()
            for name in axes:
                if name in done:
                    index.append(mine[name])
                elif name == free[0]:
                    index.append(step)
                    inner = (step,)
                else:
                    index.append(slice(None))
            index = tuple(index) + (slice(None), columns)
            value = partial[index].astype(jnp.float32)
            for offset in range(1, sizes[axis]):
                value = value + land[(offset - 1,) + inner].astype(jnp.float32)
            if free:
                partial[index] = value.astype(jnp.bfloat16)
            else:
                out_ref[:, columns] = (
                    hidden_state_ref[:, columns].astype(jnp.float32) + value
                ).astype(jnp.bfloat16)
            return _

        if free:
            lax.fori_loop(0, sizes[free[0]], add, 0)
        else:
            add(0, 0)

    slot = send_sem.shape[0] // 2
    for stage in range(4):
        for piece in range(2):
            if stage:
                for copy in pending[piece]:
                    copy.wait()
                add_landed(piece, stage - 1)
            pending[piece], slot = start_sum(piece, stage, slot)
    for piece in range(2):
        for copy in pending[piece]:
            copy.wait()
        add_landed(piece, 3)


def channel_mixer(normed, hidden_state, up_send, down_send, taps, sp_count, tp_count):
    cores = 2
    across = tp_count // cores
    deep = math.gcd(across, sp_count)
    sizes = {"z": sp_count // deep, "y": deep, "x": across, "c": cores}
    rows, width = normed.shape
    half = width // 2
    grid = tuple(sizes[name] for name in axes)
    total = math.prod(grid) * rows
    landing = []
    for order in sum_orders:
        for stage in range(4):
            axis = order[stage]
            left = tuple(sizes[name] for name in axes if name not in order[: stage + 1])
            landing.append(
                pltpu.VMEM((max(sizes[axis] - 1, 1),) + left + (rows, half), jnp.bfloat16)
            )
    copies = 2 * 2 * sum(max(sizes[name] - 1, 0) for name in axes)
    vmem = pl.BlockSpec(memory_space=pltpu.VMEM)
    return pl.pallas_call(
        lambda *refs: channel_kernel(sizes, *refs),
        name="channel_mixer",
        out_shape=jax.ShapeDtypeStruct((rows, width), jnp.bfloat16),
        in_specs=[vmem] * 5,
        out_specs=vmem,
        scratch_shapes=[
            pltpu.VMEM(grid + (rows, width), jnp.bfloat16),
            pltpu.VMEM((total + 16, up_send.shape[2]), jnp.float32),
            pltpu.VMEM(grid + (rows, width), jnp.bfloat16),
            pltpu.VMEM(up_send.shape, jnp.bfloat16),
            pltpu.VMEM(down_send.shape, jnp.bfloat16),
            pltpu.VMEM((down_send.shape[1], width), jnp.bfloat16),
            *landing,
            pltpu.SemaphoreType.DMA((3,)),
            pltpu.SemaphoreType.DMA((copies,)),
            pltpu.SemaphoreType.DMA((copies,)),
            pltpu.SemaphoreType.DMA((2, sp_count)),
            pltpu.SemaphoreType.DMA((2, sp_count)),
        ],
        compiler_params=pltpu.CompilerParams(
            collective_id=1, has_side_effects=True, vmem_limit_bytes=63 * 1024 * 1024
        ),
    )(normed, hidden_state, up_send, down_send, taps)


def turns(step_size, count):
    coarse = jnp.round(step_size * 1024.0) / 1024.0
    whole = coarse * count
    whole = whole - 2.0 * jnp.floor(whole * 0.5)
    return whole + (step_size - coarse) * count


def mixer(mixer_input, time_step, damping, input_map, readout, skip_gain):
    rows = mixer_input.shape[0]
    groups = time_step.shape[1]
    states, width = input_map.shape[3], input_map.shape[4]
    count, mine = lax.axis_size("sp"), lax.axis_index("sp")
    at = jnp.arange(rows)
    lower = at[:, None] >= at[None, :]
    reach = jnp.stack((lower, lower.T))
    log_decay = -0.5 * time_step[:, None, :] - damping
    log_sum = jnp.einsum("ktu,kug->kgt", reach.astype(jnp.float32), log_decay, precision=highest)
    weights = jnp.where(
        reach[:, None],
        jnp.exp(jnp.minimum(log_sum[:, :, :, None] - log_sum[:, :, None, :], 0.0)),
        0.0,
    )
    number = jnp.arange(states, dtype=jnp.float32)
    dt = time_step[:, :, None, None]
    angle = math.pi * turns(dt, number[None, :] * at.astype(jnp.float32)[:, None])
    sign = jnp.array([1.0, -1.0], jnp.float32)[:, None, None, None]
    cos, sin = jnp.cos(angle), jnp.sin(angle) * sign
    grouped = mixer_input.reshape(rows, groups, width)
    drive = jnp.einsum("tgh,kpgnh->kpgtn", grouped, input_map, preferred_element_type=jnp.float32)
    drive = drive * jnp.sqrt(-jnp.expm1(-time_step))[:, None, :, None, None]
    rotated = jnp.concatenate(
        (cos * drive[:, 0] + sin * drive[:, 1], cos * drive[:, 1] - sin * drive[:, 0]), axis=3
    )
    local = jnp.einsum("kgts,kgsn->kgtn", weights, rotated, precision=lax.Precision.HIGH)
    ends = jnp.stack((local[0, :, -1], local[1, :, 0]))
    totals = jnp.stack((log_sum[0, :, -1], log_sum[1, :, 0]))
    flat = ends.reshape(2 * groups, 2 * states)
    spare = jnp.pad(totals.reshape(1, 2 * groups), ((0, 7), (0, 2 * states - 2 * groups)))
    every = gather_ends(jnp.concatenate((flat, spare), axis=0), count)
    end_all = every[:, : 2 * groups].reshape(count, 2, groups, 2 * states)
    total_all = every[:, 2 * groups, : 2 * groups].reshape(count, 2, groups)
    index = jnp.arange(count)
    away = jnp.stack((mine - index, index - mine), axis=1)
    lo = jnp.minimum(index, mine)[:, None]
    hi = jnp.maximum(index, mine)[:, None]
    between = ((index[None, :] > lo) & (index[None, :] < hi)).astype(jnp.float32)
    span = jnp.einsum("ji,ikg->jkg", between, total_all, precision=highest)
    factor = jnp.where(away[:, :, None] > 0, jnp.exp(span), 0.0)
    block_turn = turns(time_step[:, :, None], number * rows)
    hop = jnp.abs(mine - index).astype(jnp.float32)[:, None, None, None] * block_turn
    hop = math.pi * (hop - 2.0 * jnp.floor(hop * 0.5))
    hop_cos, hop_sin = jnp.cos(hop) * factor[..., None], jnp.sin(hop) * factor[..., None]
    end_re, end_im = end_all[..., :states], end_all[..., states:]
    carry = jnp.concatenate(
        (
            jnp.sum(hop_cos * end_re - hop_sin * end_im, axis=0),
            jnp.sum(hop_cos * end_im + hop_sin * end_re, axis=0),
        ),
        axis=2,
    )
    local = local + jnp.exp(log_sum)[..., None] * carry[:, :, None, :]
    re, im = local[..., :states], local[..., states:]
    state = jnp.concatenate((cos * re - sin * im, cos * im + sin * re), axis=3)
    out_map = jnp.concatenate((readout[:, 0], -readout[:, 1]), axis=3)
    mixed = jnp.einsum("kgtn,kghn->tgh", state, out_map, precision=lax.Precision.HIGH)
    return mixed.reshape(rows, groups * width) + skip_gain[None, :] * mixer_input.astype(
        jnp.float32
    )


gather_paths = (("z", "y", "x"), ("z", "x", "y")) * 2
sum_paths = (("x", "y", "z"), ("y", "x", "z")) * 2
chip_axes = ("z", "y", "x")


def layer_kernel(sizes, *refs):
    (
        x_ref,
        step_ref,
        damping_ref,
        tab_ref,
        turn_ref,
        in_ref,
        readout_ref,
        vec_ref,
        taps_ref,
        residual_ref,
        channel_ref,
        out_w_hbm,
        value_hbm,
        gate_hbm,
        down_hbm,
        out_ref,
        x_t,
        decay_parts,
        local,
        carried,
        packet,
        packets,
        carry,
        y_all,
        y_land,
        vec_all,
        out_w,
        state_rows,
        taps,
        up_w,
        down_w,
        rows_all,
        up_rows,
        hidden_rows,
        partial,
    ) = refs[:35]
    pieces = len(gather_paths)
    landing = refs[35 : 35 + 3 * pieces]
    (
        local_sem,
        small_send,
        small_recv,
        taps_sem,
        hop_send,
        hop_recv,
        w_send,
        w_recv,
        f_send,
        f_recv,
    ) = refs[35 + 3 * pieces :]
    span, channels = x_ref.shape
    pairs, heads, lanes = in_ref.shape[0], in_ref.shape[1], tab_ref.shape[3]
    groups = step_ref.shape[1]
    tiles = span // 8
    rows, width = residual_ref.shape
    piece_width = width // pieces
    depth = value_hbm.shape[0]
    part = down_hbm.shape[1]
    unit = taps.shape[1]
    cores = sizes["c"]
    count, tp_count = sizes["z"] * sizes["y"], sizes["x"] * cores
    per = count // cores
    blocks = count * sizes["x"]
    sp, tp = lax.axis_index("sp"), lax.axis_index("tp")
    mine = {
        "z": sp // sizes["y"],
        "y": lax.rem(sp, sizes["y"]),
        "x": tp // cores,
        "c": lax.rem(tp, cores),
    }
    core = mine["c"]
    partner = (sp, mine["x"] * cores + lax.rem(core + 1, cores))

    def neighbour(axis, offset):
        at = dict(mine)
        at[axis] = lax.rem(mine[axis] + offset, sizes[axis])
        return at[axis], (at["z"] * sizes["y"] + at["y"], at["x"] * cores + at["c"])

    def remote(source, target, send, recv, device):
        return pltpu.make_async_remote_copy(
            src_ref=source,
            dst_ref=target,
            send_sem=send,
            recv_sem=recv,
            device_id=device,
            device_id_type=mesh_ids,
        )

    barrier = pltpu.get_barrier_semaphore()
    greeted = 0
    for offset in range(count):
        for turn in range(cores):
            if offset or turn:
                peer = lax.rem(sp + offset, count)
                other = mine["x"] * cores + lax.rem(core + turn, cores)
                pl.semaphore_signal(barrier, inc=1, device_id=(peer, other), device_id_type=mesh_ids)
                greeted += 1
    for offset in range(1, sizes["x"]):
        for turn in range(cores):
            other = lax.rem(mine["x"] + offset, sizes["x"]) * cores + turn
            pl.semaphore_signal(barrier, inc=1, device_id=(sp, other), device_id_type=mesh_ids)
            greeted += 1

    out_copy = pltpu.make_async_copy(out_w_hbm, out_w, local_sem.at[0])
    out_copy.start()
    pl.semaphore_wait(barrier, greeted)

    def block_view(kind, source):
        if kind == 2:
            return down_w.at[:, pl.ds(pl.multiple_of(source * part, part), part)]
        column = kind * unit
        return up_w.at[pl.ds(pl.multiple_of(source * depth, depth), depth), pl.ds(column, unit)]

    keeper = lax.rem(sp, cores)

    def weight_copy(kind, slot):
        place = lax.rem(slot + sp, per)
        chip = core * per + place
        start = pl.multiple_of(place * unit, unit)
        if kind == 2:
            source = down_hbm.at[pl.ds(start, unit), :]
        else:
            source = (value_hbm, gate_hbm)[kind].at[:, pl.ds(start, unit)]
        stays = (chip == sp) & (keeper == core)
        target = block_view(kind, sp)
        device = (chip, mine["x"] * cores + keeper)

        def here():
            return pltpu.make_async_copy(source, target, w_recv.at[kind, sp])

        def away():
            return remote(source, target, w_send.at[kind, slot], w_recv.at[kind, sp], device)

        return stays, here, away

    def send_weights(kinds, slots):
        for slot in slots:
            for kind in kinds:
                stays, here, away = weight_copy(kind, slot)
                pl.when(stays)(lambda: here().start())
                pl.when(jnp.logical_not(stays))(lambda: away().start())

    def finish_sends():
        for slot in range(per):
            for kind in range(3):
                stays, _, away = weight_copy(kind, slot)
                pl.when(jnp.logical_not(stays))(lambda: away().wait_send())

    def forward_weights(kinds):
        started = []
        for index in range(per):
            for kind in kinds:
                source = core + cores * index
                view = block_view(kind, source)
                remote(view, view, w_send.at[kind, 0], w_recv.at[kind, source], partner).wait_recv()
                copy = remote(view, view, f_send.at[kind, index], f_recv.at[kind, index], partner)
                copy.start()
                started.append(copy)
        return started

    def forwarded(kinds, started):
        for copy in started:
            copy.wait_send()
        for index in range(per):
            for kind in kinds:
                view = block_view(kind, lax.rem(core + 1, cores) + cores * index)
                remote(view, view, f_send.at[kind, index], f_recv.at[kind, index], partner).wait_recv()

    send_weights((0,), (0,))

    vec_copies = []
    for offset in range(1, tp_count):
        copy = remote(
            vec_ref,
            vec_all.at[tp],
            small_send.at[0, offset],
            small_recv.at[0, offset],
            (sp, lax.rem(tp + offset, tp_count)),
        )
        copy.start()
        vec_copies.append(copy)
    vec_all[tp] = vec_ref[...]

    owns_taps = core == sp // per
    taps_view = taps_ref.at[:, pl.ds(pl.multiple_of(lax.rem(sp, per) * unit, unit), unit)]
    taps_keep = pltpu.make_async_copy(taps_view, taps, taps_sem.at[0])
    taps_send = remote(taps_view, taps, taps_sem.at[1], taps_sem.at[2], partner)

    @pl.when(owns_taps)
    def _():
        taps_keep.start()
        taps_send.start()

    x_t[...] = jnp.transpose(x_ref[...].astype(jnp.float32)).astype(jnp.bfloat16)
    for k in range(2):
        left = jnp.exp(-0.5 * step_ref[k : k + 1, :] - damping_ref[k])
        for level in range(3):
            rounded = left.astype(jnp.bfloat16)
            decay_parts[k, :, level * groups : (level + 1) * groups] = rounded
            left = left - rounded.astype(jnp.float32)

    row_in_tile = lax.broadcasted_iota(jnp.int32, (1, 8, lanes), 1)
    pick_row = lax.rem(lax.broadcasted_iota(jnp.int32, (3 * groups, lanes), 0), groups)
    pick_lane = lax.broadcasted_iota(jnp.int32, (3 * groups, lanes), 1) // (lanes // 2)

    def chain(k, at, start_real, start_imag):
        real, imag = start_real, start_imag
        found = [None] * tiles
        for tile in range(tiles) if k == 0 else range(tiles - 1, -1, -1):
            place = pl.ds(tile * 8, 8)
            cos, sin = carried[at, 0, place, :], carried[at, 1, place, :]
            full_real = local[at, 0, place, :] + (cos * real - sin * imag)
            full_imag = local[at, 1, place, :] + (cos * imag + sin * real)
            found[tile] = (full_real, full_imag)
            edge = slice(7, 8) if k == 0 else slice(0, 1)
            real = jnp.broadcast_to(full_real[edge], (8, lanes))
            imag = jnp.broadcast_to(full_imag[edge], (8, lanes))
        return found, real, imag

    def first_pass(pair, _):
        inputs = x_t[pl.ds(pl.multiple_of(pair * heads, heads), heads), :]
        driven = lax.dot_general(
            inputs, in_ref[pair], (((0,), (0,)), ((), ())), preferred_element_type=jnp.float32
        )
        for k in range(2):
            at = k * pairs + pair
            pick = (pick_row == 2 * pair + pick_lane).astype(jnp.bfloat16)
            cover = jnp.dot(decay_parts[k], pick, preferred_element_type=jnp.float32)
            cover = cover.reshape(tiles, 8, lanes)
            base = 2 * k * lanes
            scale = turn_ref[2, pl.ds(at, 1), :]
            real = (driven[:, base : base + lanes] * scale).reshape(tiles, 8, lanes)
            imag = (driven[:, base + lanes : base + 2 * lanes] * scale).reshape(tiles, 8, lanes)
            for reach in (1, 2, 4):
                row = reach - 1 if k == 0 else 8 - reach
                shift = reach if k == 0 else 8 - reach
                valid = row_in_tile >= reach if k == 0 else row_in_tile < 8 - reach
                cos = tab_ref[at, 0, row : row + 1, :].reshape(1, 1, lanes)
                sin = tab_ref[at, 1, row : row + 1, :].reshape(1, 1, lanes)
                moved_real = pltpu.roll(real, shift, 1)
                moved_imag = pltpu.roll(imag, shift, 1)
                decay = jnp.where(valid, cover, 0.0)
                real = real + decay * (cos * moved_real - sin * moved_imag)
                imag = imag + decay * (cos * moved_imag + sin * moved_real)
                cover = cover * jnp.where(valid, pltpu.roll(cover, shift, 1), 1.0)
            local[at, 0] = real.reshape(span, lanes)
            local[at, 1] = imag.reshape(span, lanes)
            carried[at, 0] = (cover * tab_ref[at, 0].reshape(1, 8, lanes)).reshape(span, lanes)
            carried[at, 1] = (cover * tab_ref[at, 1].reshape(1, 8, lanes)).reshape(span, lanes)
        for k in range(2):
            at = k * pairs + pair
            none = jnp.zeros((8, lanes), jnp.float32)
            real, imag = chain(k, at, none, none)[1:]
            packet[pl.ds(at, 1), :] = real[0:1]
            packet[pl.ds(2 * pairs + at, 1), :] = imag[0:1]
        return _

    packet[pl.ds(4 * pairs, 2 * pairs), :] = turn_ref[3]
    lax.fori_loop(0, pairs, first_pass, 0)

    packets[sp] = packet[...]
    carry_copies = []
    for offset in range(1, count):
        copy = remote(
            packet,
            packets.at[sp],
            small_send.at[1, offset],
            small_recv.at[1, offset],
            (lax.rem(sp + offset, count), tp),
        )
        copy.start()
        carry_copies.append(copy)
    send_weights((1,), (0,))
    send_weights((0, 1), (1,))
    for copy in carry_copies:
        copy.wait()

    for k in range(2):
        at = pl.ds(k * pairs, pairs)
        cos, sin = turn_ref[0, at, :], turn_ref[1, at, :]
        real = jnp.zeros((pairs, lanes), jnp.float32)
        imag = real
        for index in range(count) if k == 0 else range(count - 1, -1, -1):
            total = packets[index, pl.ds((4 + k) * pairs, pairs), :]
            turned_real = cos * real - sin * imag
            turned_imag = cos * imag + sin * real
            before = (index < sp) if k == 0 else (index > sp)
            real = jnp.where(before, packets[index, at, :] + total * turned_real, real)
            imag = jnp.where(
                before,
                packets[index, pl.ds((2 + k) * pairs, pairs), :] + total * turned_imag,
                imag,
            )
        carry[0, at, :] = real
        carry[1, at, :] = imag

    gains = vec_ref[1:2, :] * x_ref[...].astype(jnp.float32)
    for pair in range(pairs):
        parts = []
        for k in range(2):
            at = k * pairs + pair
            real = jnp.broadcast_to(carry[0, at : at + 1, :], (8, lanes))
            imag = jnp.broadcast_to(carry[1, at : at + 1, :], (8, lanes))
            found, _, _ = chain(k, at, real, imag)
            parts.append(jnp.concatenate([item[0] for item in found], axis=0))
            parts.append(jnp.concatenate([item[1] for item in found], axis=0))
        state = jnp.concatenate(parts, axis=1)
        state_high = state.astype(jnp.bfloat16)
        state_low = (state - state_high.astype(jnp.float32)).astype(jnp.bfloat16)
        out_map = readout_ref[pair]
        map_high = out_map.astype(jnp.bfloat16)
        map_low = (out_map - map_high.astype(jnp.float32)).astype(jnp.bfloat16)

        def apply(left, right):
            return lax.dot_general(
                left, right, (((1,), (1,)), ((), ())), preferred_element_type=jnp.float32
            )

        both = apply(state_high, jnp.concatenate((map_high, map_low), axis=0))
        mixed = both[:, :heads] + both[:, heads:] + apply(state_low, map_high)
        columns = slice(pair * heads, (pair + 1) * heads)
        y_all[:, columns] = mixed + gains[:, columns]
    y_copies = []
    for offset in range(1, tp_count):
        peer = lax.rem(tp + offset, tp_count)
        copy = remote(
            y_all.at[pl.ds(pl.multiple_of(peer * rows, rows), rows), :],
            y_land.at[tp],
            small_send.at[2, offset],
            small_recv.at[2, offset],
            (sp, peer),
        )
        copy.start()
        y_copies.append(copy)
    y_land[tp] = y_all[pl.ds(pl.multiple_of(tp * rows, rows), rows), :]
    for copy in vec_copies + y_copies:
        copy.wait()
    out_copy.wait()

    mixed = jnp.concatenate([y_land[peer] for peer in range(tp_count)], axis=1)
    gain = jnp.concatenate([vec_all[peer, 0:1, :] for peer in range(tp_count)], axis=1)
    inverse = lax.rsqrt(jnp.mean(mixed * mixed, axis=1, keepdims=True) + norm_eps)
    normed_mix = (mixed * inverse * gain).astype(jnp.bfloat16)
    square = jnp.zeros((rows, 1), jnp.float32)
    tile = 512
    for start in range(0, width, tile):
        columns = pl.ds(start, tile)
        mixed_rows = jnp.dot(normed_mix, out_w[:, columns], preferred_element_type=jnp.float32)
        summed = (residual_ref[:, columns].astype(jnp.float32) + mixed_rows).astype(jnp.bfloat16)
        state_rows[:, columns] = summed
        wide = summed.astype(jnp.float32)
        square = square + jnp.sum(wide * wide, axis=1, keepdims=True)
    scale_rows = lax.rsqrt(square / width + norm_eps)
    normed = state_rows[...].astype(jnp.float32) * scale_rows * channel_ref[...]
    rows_all[mine["z"], mine["y"], mine["x"]] = normed.astype(jnp.bfloat16)

    slot = 0
    pending = [[] for _ in range(pieces)]
    for stage in range(3):
        for piece in range(pieces):
            axis = gather_paths[piece][stage]
            done = gather_paths[piece][:stage]
            for copy in pending[piece]:
                copy.wait()
            pending[piece] = []
            index = tuple(slice(None) if name in done else mine[name] for name in chip_axes)
            block = rows_all.at[index + (slice(None), pl.ds(piece * piece_width, piece_width))]
            for offset in range(1, sizes[axis]):
                _, device = neighbour(axis, offset)
                copy = remote(block, block, hop_send.at[slot], hop_recv.at[slot], device)
                copy.start()
                pending[piece].append(copy)
                slot += 1
        if stage == 0:
            send_weights((0, 1), range(2, per))
            send_weights((2,), range(per))
    up_started = forward_weights((0, 1))
    for piece in range(pieces):
        for copy in pending[piece]:
            copy.wait()
    forwarded((0, 1), up_started)

    @pl.when(core == 0)
    def _():
        up_rows[1, pl.ds(0, 8), :] = jnp.zeros((8, 2 * unit), jnp.float32)

    @pl.when(core == cores - 1)
    def _():
        up_rows[blocks, pl.ds(rows + 8, 8), :] = jnp.zeros((8, 2 * unit), jnp.float32)

    chunk = 256

    def project(n, _):
        columns = pl.ds(pl.multiple_of(n * chunk, chunk), chunk)
        block = rows_all[...].reshape(blocks * rows, width)
        up = jnp.dot(block, up_w[:, columns], preferred_element_type=jnp.float32)
        up = up.astype(jnp.bfloat16).astype(jnp.float32)
        up_rows[pl.ds(1, blocks), pl.ds(8, rows), columns] = up.reshape(blocks, rows, chunk)
        return _

    lax.fori_loop(0, 2 * unit // chunk, project, 0)

    edges = []
    for kind, (take, land, first) in enumerate(((rows, 0, 1 + core), (8, rows + 8, core))):
        copy = remote(
            up_rows.at[pl.ds(1, blocks), pl.ds(take, 8), :],
            up_rows.at[pl.ds(first, blocks), pl.ds(land, 8), :],
            small_send.at[3, kind],
            small_recv.at[3, kind],
            partner,
        )
        copy.start()
        edges.append(copy)
    down_started = forward_weights((2,))

    @pl.when(owns_taps)
    def _():
        taps_keep.wait()
        taps_send.wait_send()

    @pl.when(jnp.logical_not(owns_taps))
    def _():
        taps_send.wait_recv()

    for copy in edges:
        copy.wait()

    def mix(b, _):
        window = up_rows[b + 1]

        def conv(base, columns):
            return (
                taps[base : base + 1, :] * window[7 : rows + 7, columns]
                + taps[base + 1 : base + 2, :] * window[8 : rows + 8, columns]
                + taps[base + 2 : base + 3, :] * window[9 : rows + 9, columns]
            )

        value = conv(0, slice(0, unit))
        gate = conv(3, slice(unit, 2 * unit))
        hidden = value * (gate / (1.0 + jnp.exp(-gate)))
        hidden_rows[pl.ds(pl.multiple_of(b * rows, rows), rows), :] = hidden.astype(jnp.bfloat16)
        return _

    lax.fori_loop(0, blocks, mix, 0)
    forwarded((2,), down_started)

    def start_sum(piece, stage, slot):
        axis = sum_paths[piece][stage]
        done = sum_paths[piece][:stage]
        started = []
        for offset in range(1, sizes[axis]):
            place, device = neighbour(axis, offset)
            index = tuple(
                place if name == axis else mine[name] if name in done else slice(None)
                for name in chip_axes
            )
            copy = remote(
                partial.at[index + (slice(None), pl.ds(piece * piece_width, piece_width))],
                landing[piece * 3 + stage].at[offset - 1],
                hop_send.at[slot],
                hop_recv.at[slot],
                device,
            )
            copy.start()
            started.append(copy)
            slot += 1
        return started, slot

    def add_landed(piece, stage):
        axis = sum_paths[piece][stage]
        done = sum_paths[piece][: stage + 1]
        land = landing[piece * 3 + stage]
        columns = pl.ds(piece * piece_width, piece_width)
        free = [name for name in chip_axes if name not in done]

        def add(step, _):
            index, inner = [], ()
            for name in chip_axes:
                if name in done:
                    index.append(mine[name])
                elif name == free[0]:
                    index.append(step)
                    inner = (step,)
                else:
                    index.append(slice(None))
            index = tuple(index) + (slice(None), columns)
            value = partial[index].astype(jnp.float32)
            for offset in range(1, sizes[axis]):
                value = value + land[(offset - 1,) + inner].astype(jnp.float32)
            if free:
                partial[index] = value.astype(jnp.bfloat16)
            else:
                out_ref[:, columns] = (
                    state_rows[:, columns].astype(jnp.float32) + value
                ).astype(jnp.bfloat16)
            return _

        if free:
            lax.fori_loop(0, sizes[free[0]], add, 0)
        else:
            add(0, 0)

    slot = hop_send.shape[0] // 2
    pending = []
    for piece in range(pieces):
        columns = pl.ds(piece * piece_width, piece_width)
        sums = jnp.dot(hidden_rows[...], down_w[:, columns], preferred_element_type=jnp.float32)
        shape = partial.shape[:3] + (rows, piece_width)
        partial[:, :, :, :, columns] = sums.astype(jnp.bfloat16).reshape(shape)
        started, slot = start_sum(piece, 0, slot)
        pending.append(started)
    for stage in range(1, 3):
        for piece in range(pieces):
            for copy in pending[piece]:
                copy.wait()
            add_landed(piece, stage - 1)
            pending[piece], slot = start_sum(piece, stage, slot)
    for piece in range(pieces):
        for copy in pending[piece]:
            copy.wait()
        add_landed(piece, 2)
    finish_sends()


def whole_layer(sizes, arrays, weights, unit):
    x, time_step, _, tab, turn, in_map, _, vec, taps, residual, _ = arrays
    out_weight, value_weight, gate_weight, down_weight = weights
    span, channels = x.shape
    groups, lanes = time_step.shape[1], tab.shape[3]
    chains = turn.shape[1]
    rows, width = residual.shape
    pieces = len(gather_paths)
    count, tp_count = sizes["z"] * sizes["y"], sizes["x"] * sizes["c"]
    grid = tuple(sizes[name] for name in chip_axes)
    blocks = math.prod(grid)
    per = count // sizes["c"]
    landing = []
    for order in sum_paths:
        for stage in range(3):
            axis = order[stage]
            left = tuple(sizes[name] for name in chip_axes if name not in order[: stage + 1])
            landing.append(
                pltpu.VMEM((max(sizes[axis] - 1, 1),) + left + (rows, width // pieces), jnp.bfloat16)
            )
    copies = 2 * pieces * sum(max(sizes[name] - 1, 0) for name in chip_axes)
    small = max(count, tp_count)
    vmem = pl.BlockSpec(memory_space=pltpu.VMEM)
    far = pl.BlockSpec(memory_space=pl.ANY)
    dma = pltpu.SemaphoreType.DMA
    f32, bf16 = jnp.float32, jnp.bfloat16
    return pl.pallas_call(
        lambda *refs: layer_kernel(sizes, *refs),
        name="whole_layer",
        out_shape=jax.ShapeDtypeStruct((rows, width), bf16),
        in_specs=[vmem] * 11 + [far] * 4,
        out_specs=vmem,
        scratch_shapes=[
            pltpu.VMEM((channels, span), bf16),
            pltpu.VMEM((2, span, 3 * groups), bf16),
            pltpu.VMEM((chains, 2, span, lanes), f32),
            pltpu.VMEM((chains, 2, span, lanes), f32),
            pltpu.VMEM((3 * chains, lanes), f32),
            pltpu.VMEM((count, 3 * chains, lanes), f32),
            pltpu.VMEM((2, chains, lanes), f32),
            pltpu.VMEM((span, channels), f32),
            pltpu.VMEM((tp_count, rows, channels), f32),
            pltpu.VMEM((tp_count,) + vec.shape, f32),
            pltpu.VMEM(out_weight.shape, bf16),
            pltpu.VMEM((rows, width), bf16),
            pltpu.VMEM((taps.shape[0], unit), f32),
            pltpu.VMEM((width, 2 * unit), bf16),
            pltpu.VMEM((unit, width), bf16),
            pltpu.VMEM(grid + (rows, width), bf16),
            pltpu.VMEM((blocks + 2, rows + 16, 2 * unit), f32),
            pltpu.VMEM((blocks * rows, unit), bf16),
            pltpu.VMEM(grid + (rows, width), bf16),
            *landing,
            dma((1,)),
            dma((4, small)),
            dma((4, small)),
            dma((3,)),
            dma((copies,)),
            dma((copies,)),
            dma((3, per)),
            dma((3, count)),
            dma((3, per)),
            dma((3, per)),
        ],
        compiler_params=pltpu.CompilerParams(
            collective_id=2, has_side_effects=True, vmem_limit_bytes=63 * 1024 * 1024
        ),
    )(*arrays, *weights)


def mesh_sizes(sp_count, tp_count):
    cores = 2
    across = tp_count // cores
    deep = math.gcd(across, sp_count)
    return {"z": sp_count // deep, "y": deep, "x": across, "c": cores}


def tile_units(sizes, x_shape, in_shape, value_shape, down_shape, residual_shape):
    count = sizes["z"] * sizes["y"]
    unit = value_shape[1] * sizes["c"] // count
    rows, width = residual_shape
    span, states, head = x_shape[0], in_shape[3], in_shape[4]
    fits = (
        count % sizes["c"] == 0
        and unit % 128 == 0
        and 2 * unit % 256 == 0
        and value_shape[0] % 16 == 0
        and down_shape[1] % 128 == 0
        and width % 512 == 0
        and rows % 16 == 0
        and span % 128 == 0
        and 2 * states == 128
        and in_shape[2] % 16 == 0
        and width % (256 * len(gather_paths)) == 0
        and head % 16 == 0
        and x_shape[1] % 128 == 0
    )
    return unit if fits else 0


def one_kernel(sizes, unit, args):
    (
        mixer_input,
        time_step,
        damping,
        input_map,
        readout,
        skip_gain,
        out_gain,
        out_weight,
        residual,
        channel_gain,
        value_weight,
        gate_weight,
        value_taps,
        gate_taps,
        down_weight,
    ) = args
    span = mixer_input.shape[0]
    groups, states, head = input_map.shape[2:]
    pairs = groups // 2
    number = jnp.arange(states, dtype=jnp.float32)

    def by_pair(array):
        return array.reshape(2 * pairs, 2 * array.shape[-1])

    near = jnp.arange(1, 9, dtype=jnp.float32)
    reach = jnp.stack((near, near[::-1]))[:, :, None, None] * number
    angle = math.pi * turns(time_step[:, None, :, None], reach)
    tab = jnp.stack((jnp.cos(angle), jnp.sin(angle)))
    tab = tab.reshape(2, 2, 8, pairs, 2 * states).transpose(1, 3, 0, 2, 4)
    tab = tab.reshape(2 * pairs, 2, 8, 2 * states)
    far = math.pi * turns(time_step[:, :, None], number * span)
    scale = jnp.sqrt(-jnp.expm1(-time_step))
    total = jnp.exp(-0.5 * span * time_step - jnp.sum(damping, axis=1))
    turn = jnp.stack(
        [
            by_pair(jnp.broadcast_to(item, far.shape))
            for item in (jnp.cos(far), jnp.sin(far), scale[:, :, None], total[:, :, None])
        ]
    )
    same = jnp.eye(2, dtype=jnp.float32)
    in_map = input_map.reshape(2, 2, pairs, 2, states, head).transpose(2, 3, 5, 0, 1, 4)
    in_map = in_map[:, :, :, :, :, None, :] * same[:, None, None, None, :, None].astype(
        in_map.dtype
    )
    in_map = in_map.reshape(pairs, 2 * head, 8 * states)
    signed = jnp.stack((readout[:, 0], -readout[:, 1]), axis=1)
    out_map = signed.reshape(2, 2, pairs, 2, head, states).transpose(2, 3, 4, 0, 1, 5)
    out_map = out_map[:, :, :, :, :, None, :] * same[:, None, None, None, :, None]
    out_map = out_map.reshape(pairs, 2 * head, 8 * states)
    vec = jnp.pad(jnp.stack((out_gain, skip_gain)), ((0, 6), (0, 0)))
    taps = jnp.pad(jnp.concatenate((value_taps, gate_taps)), ((0, 2), (0, 0)))
    arrays = (
        mixer_input,
        time_step,
        damping,
        tab,
        turn,
        in_map,
        out_map,
        vec,
        taps,
        residual,
        channel_gain.reshape(1, -1),
    )
    return whole_layer(
        sizes, arrays, (out_weight, value_weight, gate_weight, down_weight), unit
    )


def body(
    mixer_input,
    time_step,
    damping,
    input_map,
    readout,
    skip_gain,
    out_gain,
    out_weight,
    residual,
    channel_gain,
    value_weight,
    gate_weight,
    value_taps,
    gate_taps,
    down_weight,
):
    count, mine = lax.axis_size("sp"), lax.axis_index("sp")
    sizes = mesh_sizes(count, lax.axis_size("tp"))
    unit = tile_units(
        sizes,
        mixer_input.shape,
        input_map.shape,
        value_weight.shape,
        down_weight.shape,
        residual.shape,
    )
    if unit:
        args = (mixer_input, time_step, damping, input_map, readout, skip_gain, out_gain)
        args += (out_weight, residual, channel_gain, value_weight, gate_weight)
        return one_kernel(sizes, unit, args + (value_taps, gate_taps, down_weight))
    depth, hidden_width = value_weight.shape
    part = hidden_width // count
    up_send = jnp.concatenate(
        (
            value_weight.reshape(depth, count, part).swapaxes(0, 1),
            gate_weight.reshape(depth, count, part).swapaxes(0, 1),
        ),
        axis=2,
    )
    down_send = down_weight.reshape(count, part, down_weight.shape[1])
    mixed_y = mixer(mixer_input, time_step, damping, input_map, readout, skip_gain)
    tp_count = lax.axis_size("tp")
    mixed_y = mixed_y.reshape(tp_count, -1, out_gain.shape[0])
    gain_row = jnp.broadcast_to(out_gain, (tp_count, 1, out_gain.shape[0]))
    mixed_y = jnp.concatenate((mixed_y, gain_row), axis=1)
    mixed_y = lax.all_to_all(mixed_y, "tp", split_axis=0, concat_axis=0, tiled=True)
    mixed_y = mixed_y.swapaxes(0, 1).reshape(mixed_y.shape[1], -1)
    mixed_y, gain = mixed_y[:-1], mixed_y[-1]
    inverse = lax.rsqrt(jnp.mean(mixed_y * mixed_y, axis=1, keepdims=True) + norm_eps)
    normed_mix = (mixed_y * inverse * gain[None, :]).astype(jnp.bfloat16)
    mixed_rows = jnp.dot(normed_mix, out_weight, preferred_element_type=jnp.float32)
    hidden_state = (residual.astype(jnp.float32) + mixed_rows).astype(jnp.bfloat16)
    state_wide = hidden_state.astype(jnp.float32)
    scale_rows = lax.rsqrt(jnp.mean(state_wide * state_wide, axis=1, keepdims=True) + norm_eps)
    normed = (state_wide * scale_rows * channel_gain[None, :]).astype(jnp.bfloat16)
    taps = jnp.concatenate(
        (
            lax.dynamic_slice_in_dim(value_taps, mine * part, part, axis=1),
            lax.dynamic_slice_in_dim(gate_taps, mine * part, part, axis=1),
        ),
        axis=1,
    )
    return channel_mixer(normed, hidden_state, up_send, down_send, taps, count, tp_count)


def solution(mesh):
    in_specs = (
        P("sp", "tp"),
        P(None, "tp"),
        P(None, "sp", "tp"),
        P(None, None, "tp", None, None),
        P(None, None, "tp", None, None),
        P("tp"),
        P("tp"),
        P(),
        P(("sp", "tp"), None),
        P(),
        P("sp", "tp"),
        P("sp", "tp"),
        P(None, "tp"),
        P(None, "tp"),
        P("tp", "sp"),
    )
    out_specs = P(("sp", "tp"), None)
    return jax.shard_map(body, mesh=mesh, in_specs=in_specs, out_specs=out_specs, check_vma=False)
```

```python
import math

import jax
import jax.numpy as jnp
from jax import lax
from jax.experimental import pallas as pl
from jax.experimental.pallas import tpu as pltpu
from jax.sharding import PartitionSpec as P

norm_eps = 1e-06
highest = lax.Precision.HIGHEST
mesh_ids = pl.DeviceIdType.MESH


def carry_kernel(count, own_ref, all_ref, local_sem, send_sem, recv_sem):
    sp, tp = lax.axis_index("sp"), lax.axis_index("tp")
    barrier = pltpu.get_barrier_semaphore()
    for offset in range(1, count):
        peer = lax.rem(sp + offset, count)
        pl.semaphore_signal(barrier, inc=1, device_id=(peer, tp), device_id_type=mesh_ids)
    pl.semaphore_wait(barrier, count - 1)
    keep = pltpu.make_async_copy(own_ref, all_ref.at[sp], local_sem)
    keep.start()
    copies = []
    for offset in range(1, count):
        peer = lax.rem(sp + offset, count)
        copy = pltpu.make_async_remote_copy(
            src_ref=own_ref,
            dst_ref=all_ref.at[sp],
            send_sem=send_sem.at[offset],
            recv_sem=recv_sem.at[offset],
            device_id=(peer, tp),
            device_id_type=mesh_ids,
        )
        copy.start()
        copies.append(copy)
    keep.wait()
    for copy in copies:
        copy.wait()


def gather_ends(packed, count):
    vmem = pl.BlockSpec(memory_space=pltpu.VMEM)
    return pl.pallas_call(
        lambda *refs: carry_kernel(count, *refs),
        name="gather_ends",
        out_shape=jax.ShapeDtypeStruct((count,) + packed.shape, packed.dtype),
        in_specs=[vmem],
        out_specs=vmem,
        scratch_shapes=[
            pltpu.SemaphoreType.DMA,
            pltpu.SemaphoreType.DMA((count,)),
            pltpu.SemaphoreType.DMA((count,)),
        ],
        compiler_params=pltpu.CompilerParams(collective_id=0, has_side_effects=True),
    )(packed)


gather_orders = (("z", "y", "x", "c"), ("y", "z", "x", "c"))
sum_orders = (("c", "x", "y", "z"), ("c", "z", "y", "x"))
axes = ("z", "y", "x", "c")


def channel_kernel(sizes, *refs):
    normed_ref, hidden_state_ref, up_send, down_send, taps_ref, out_ref = refs[:6]
    rows_all, up_rows, partial, up_land, down_land, down_ref = refs[6:12]
    landing = refs[12:20]
    local_sem, send_sem, recv_sem, weight_send_sem, weight_recv_sem = refs[20:25]
    rows, width = normed_ref.shape
    half = width // 2
    count, part, part_width = down_send.shape
    sp, tp = lax.axis_index("sp"), lax.axis_index("tp")
    mine = {
        "z": sp // sizes["y"],
        "y": lax.rem(sp, sizes["y"]),
        "x": tp // sizes["c"],
        "c": lax.rem(tp, sizes["c"]),
    }

    def neighbour(axis, offset):
        at = dict(mine)
        at[axis] = lax.rem(mine[axis] + offset, sizes[axis])
        return at[axis], (at["z"] * sizes["y"] + at["y"], at["x"] * sizes["c"] + at["c"])

    barrier = pltpu.get_barrier_semaphore()
    greeted = 0
    for axis in ("x", "c"):
        for offset in range(1, sizes[axis]):
            _, device = neighbour(axis, offset)
            pl.semaphore_signal(barrier, inc=1, device_id=device, device_id_type=mesh_ids)
            greeted += 1
    for offset in range(1, count):
        peer = lax.rem(sp + offset, count)
        pl.semaphore_signal(barrier, inc=1, device_id=(peer, tp), device_id_type=mesh_ids)
        greeted += 1
    pl.semaphore_wait(barrier, greeted)

    keeps = []
    for kind, (source, target) in enumerate(
        (
            (normed_ref, rows_all.at[mine["z"], mine["y"], mine["x"], mine["c"]]),
            (up_send.at[sp], up_land.at[sp]),
            (down_send.at[sp], down_land.at[sp]),
        )
    ):
        keep = pltpu.make_async_copy(source, target, local_sem.at[kind])
        keep.start()
        keeps.append(keep)
    keeps[0].wait()

    def spread(source, land, kind):
        started = []
        for offset in range(1, count):
            peer = lax.rem(sp + offset, count)
            copy = pltpu.make_async_remote_copy(
                src_ref=source.at[peer],
                dst_ref=land.at[sp],
                send_sem=weight_send_sem.at[kind, offset],
                recv_sem=weight_recv_sem.at[kind, offset],
                device_id=(peer, tp),
                device_id_type=mesh_ids,
            )
            copy.start()
            started.append(copy)
        return started

    slot = 0
    pending = [[], []]
    up_copies, down_copies = [], []
    for stage in range(4):
        if stage == 2:
            up_copies = spread(up_send, up_land, 0)
            down_copies = spread(down_send, down_land, 1)
        for piece in range(2):
            axis = gather_orders[piece][stage]
            done = gather_orders[piece][:stage]
            for copy in pending[piece]:
                copy.wait()
            pending[piece] = []
            index = tuple(slice(None) if name in done else mine[name] for name in axes)
            block = rows_all.at[index + (slice(None), pl.ds(piece * half, half))]
            for offset in range(1, sizes[axis]):
                _, device = neighbour(axis, offset)
                copy = pltpu.make_async_remote_copy(
                    src_ref=block,
                    dst_ref=block,
                    send_sem=send_sem.at[slot],
                    recv_sem=recv_sem.at[slot],
                    device_id=device,
                    device_id_type=mesh_ids,
                )
                copy.start()
                pending[piece].append(copy)
                slot += 1
    for piece in range(2):
        for copy in pending[piece]:
            copy.wait()

    plane = sizes["y"] * sizes["x"] * sizes["c"] * rows
    total = plane * sizes["z"]
    for copy in [keeps[1]] + up_copies:
        copy.wait()
    edge = jnp.zeros((8, up_rows.shape[1]), jnp.float32)
    up_rows[pl.ds(0, 8), :] = edge
    up_rows[pl.ds(total + 8, 8), :] = edge

    def project(z, _):
        block = rows_all[z].reshape(plane, width)
        up_weight = up_land[...].reshape(width, 2 * part)
        up = jnp.dot(block, up_weight, preferred_element_type=jnp.float32)
        start = pl.multiple_of(z * plane + 8, 8)
        up_rows[pl.ds(start, plane), :] = up.astype(jnp.bfloat16).astype(jnp.float32)
        return _

    lax.fori_loop(0, sizes["z"], project, 0)

    for copy in [keeps[2]] + down_copies:
        copy.wait()
    for source in range(count):
        down_ref[:, source * part_width : (source + 1) * part_width] = down_land[source]

    def mix(z, _):
        start = pl.multiple_of(z * plane, 8)
        window = up_rows[pl.ds(start, plane + 16), :]
        convolved = (
            taps_ref[0:1, :] * window[7 : plane + 7]
            + taps_ref[1:2, :] * window[8 : plane + 8]
            + taps_ref[2:3, :] * window[9 : plane + 9]
        )
        gate = convolved[:, part:]
        hidden = convolved[:, :part] * (gate / (1.0 + jnp.exp(-gate)))
        sums = jnp.dot(
            hidden.astype(jnp.bfloat16), down_ref[...], preferred_element_type=jnp.float32
        )
        partial[z] = sums.astype(jnp.bfloat16).reshape(partial.shape[1:])
        return _

    lax.fori_loop(0, sizes["z"], mix, 0)

    def start_sum(piece, stage, slot):
        axis = sum_orders[piece][stage]
        done = sum_orders[piece][:stage]
        started = []
        for offset in range(1, sizes[axis]):
            place, device = neighbour(axis, offset)
            index = tuple(
                place if name == axis else mine[name] if name in done else slice(None)
                for name in axes
            )
            copy = pltpu.make_async_remote_copy(
                src_ref=partial.at[index + (slice(None), pl.ds(piece * half, half))],
                dst_ref=landing[piece * 4 + stage].at[offset - 1],
                send_sem=send_sem.at[slot],
                recv_sem=recv_sem.at[slot],
                device_id=device,
                device_id_type=mesh_ids,
            )
            copy.start()
            started.append(copy)
            slot += 1
        return started, slot

    def add_landed(piece, stage):
        axis = sum_orders[piece][stage]
        done = sum_orders[piece][: stage + 1]
        land = landing[piece * 4 + stage]
        columns = pl.ds(piece * half, half)
        free = [name for name in axes if name not in done]

        def add(step, _):
            index, inner = [], ()
            for name in axes:
                if name in done:
                    index.append(mine[name])
                elif name == free[0]:
                    index.append(step)
                    inner = (step,)
                else:
                    index.append(slice(None))
            index = tuple(index) + (slice(None), columns)
            value = partial[index].astype(jnp.float32)
            for offset in range(1, sizes[axis]):
                value = value + land[(offset - 1,) + inner].astype(jnp.float32)
            if free:
                partial[index] = value.astype(jnp.bfloat16)
            else:
                out_ref[:, columns] = (
                    hidden_state_ref[:, columns].astype(jnp.float32) + value
                ).astype(jnp.bfloat16)
            return _

        if free:
            lax.fori_loop(0, sizes[free[0]], add, 0)
        else:
            add(0, 0)

    slot = send_sem.shape[0] // 2
    for stage in range(4):
        for piece in range(2):
            if stage:
                for copy in pending[piece]:
                    copy.wait()
                add_landed(piece, stage - 1)
            pending[piece], slot = start_sum(piece, stage, slot)
    for piece in range(2):
        for copy in pending[piece]:
            copy.wait()
        add_landed(piece, 3)


def channel_mixer(normed, hidden_state, up_send, down_send, taps, sp_count, tp_count):
    cores = 2
    across = tp_count // cores
    deep = math.gcd(across, sp_count)
    sizes = {"z": sp_count // deep, "y": deep, "x": across, "c": cores}
    rows, width = normed.shape
    half = width // 2
    grid = tuple(sizes[name] for name in axes)
    total = math.prod(grid) * rows
    landing = []
    for order in sum_orders:
        for stage in range(4):
            axis = order[stage]
            left = tuple(sizes[name] for name in axes if name not in order[: stage + 1])
            landing.append(
                pltpu.VMEM((max(sizes[axis] - 1, 1),) + left + (rows, half), jnp.bfloat16)
            )
    copies = 2 * 2 * sum(max(sizes[name] - 1, 0) for name in axes)
    vmem = pl.BlockSpec(memory_space=pltpu.VMEM)
    return pl.pallas_call(
        lambda *refs: channel_kernel(sizes, *refs),
        name="channel_mixer",
        out_shape=jax.ShapeDtypeStruct((rows, width), jnp.bfloat16),
        in_specs=[vmem] * 5,
        out_specs=vmem,
        scratch_shapes=[
            pltpu.VMEM(grid + (rows, width), jnp.bfloat16),
            pltpu.VMEM((total + 16, up_send.shape[2]), jnp.float32),
            pltpu.VMEM(grid + (rows, width), jnp.bfloat16),
            pltpu.VMEM(up_send.shape, jnp.bfloat16),
            pltpu.VMEM(down_send.shape, jnp.bfloat16),
            pltpu.VMEM((down_send.shape[1], width), jnp.bfloat16),
            *landing,
            pltpu.SemaphoreType.DMA((3,)),
            pltpu.SemaphoreType.DMA((copies,)),
            pltpu.SemaphoreType.DMA((copies,)),
            pltpu.SemaphoreType.DMA((2, sp_count)),
            pltpu.SemaphoreType.DMA((2, sp_count)),
        ],
        compiler_params=pltpu.CompilerParams(
            collective_id=1, has_side_effects=True, vmem_limit_bytes=63 * 1024 * 1024
        ),
    )(normed, hidden_state, up_send, down_send, taps)


def turns(step_size, count):
    coarse = jnp.round(step_size * 1024.0) / 1024.0
    whole = coarse * count
    whole = whole - 2.0 * jnp.floor(whole * 0.5)
    return whole + (step_size - coarse) * count


def mixer(mixer_input, time_step, damping, input_map, readout, skip_gain):
    rows = mixer_input.shape[0]
    groups = time_step.shape[1]
    states, width = input_map.shape[3], input_map.shape[4]
    count, mine = lax.axis_size("sp"), lax.axis_index("sp")
    at = jnp.arange(rows)
    lower = at[:, None] >= at[None, :]
    reach = jnp.stack((lower, lower.T))
    log_decay = -0.5 * time_step[:, None, :] - damping
    log_sum = jnp.einsum("ktu,kug->kgt", reach.astype(jnp.float32), log_decay, precision=highest)
    weights = jnp.where(
        reach[:, None],
        jnp.exp(jnp.minimum(log_sum[:, :, :, None] - log_sum[:, :, None, :], 0.0)),
        0.0,
    )
    number = jnp.arange(states, dtype=jnp.float32)
    dt = time_step[:, :, None, None]
    angle = math.pi * turns(dt, number[None, :] * at.astype(jnp.float32)[:, None])
    sign = jnp.array([1.0, -1.0], jnp.float32)[:, None, None, None]
    cos, sin = jnp.cos(angle), jnp.sin(angle) * sign
    grouped = mixer_input.reshape(rows, groups, width)
    drive = jnp.einsum("tgh,kpgnh->kpgtn", grouped, input_map, preferred_element_type=jnp.float32)
    drive = drive * jnp.sqrt(-jnp.expm1(-time_step))[:, None, :, None, None]
    rotated = jnp.concatenate(
        (cos * drive[:, 0] + sin * drive[:, 1], cos * drive[:, 1] - sin * drive[:, 0]), axis=3
    )
    local = jnp.einsum("kgts,kgsn->kgtn", weights, rotated, precision=lax.Precision.HIGH)
    ends = jnp.stack((local[0, :, -1], local[1, :, 0]))
    totals = jnp.stack((log_sum[0, :, -1], log_sum[1, :, 0]))
    flat = ends.reshape(2 * groups, 2 * states)
    spare = jnp.pad(totals.reshape(1, 2 * groups), ((0, 7), (0, 2 * states - 2 * groups)))
    every = gather_ends(jnp.concatenate((flat, spare), axis=0), count)
    end_all = every[:, : 2 * groups].reshape(count, 2, groups, 2 * states)
    total_all = every[:, 2 * groups, : 2 * groups].reshape(count, 2, groups)
    index = jnp.arange(count)
    away = jnp.stack((mine - index, index - mine), axis=1)
    lo = jnp.minimum(index, mine)[:, None]
    hi = jnp.maximum(index, mine)[:, None]
    between = ((index[None, :] > lo) & (index[None, :] < hi)).astype(jnp.float32)
    span = jnp.einsum("ji,ikg->jkg", between, total_all, precision=highest)
    factor = jnp.where(away[:, :, None] > 0, jnp.exp(span), 0.0)
    block_turn = turns(time_step[:, :, None], number * rows)
    hop = jnp.abs(mine - index).astype(jnp.float32)[:, None, None, None] * block_turn
    hop = math.pi * (hop - 2.0 * jnp.floor(hop * 0.5))
    hop_cos, hop_sin = jnp.cos(hop) * factor[..., None], jnp.sin(hop) * factor[..., None]
    end_re, end_im = end_all[..., :states], end_all[..., states:]
    carry = jnp.concatenate(
        (
            jnp.sum(hop_cos * end_re - hop_sin * end_im, axis=0),
            jnp.sum(hop_cos * end_im + hop_sin * end_re, axis=0),
        ),
        axis=2,
    )
    local = local + jnp.exp(log_sum)[..., None] * carry[:, :, None, :]
    re, im = local[..., :states], local[..., states:]
    state = jnp.concatenate((cos * re - sin * im, cos * im + sin * re), axis=3)
    out_map = jnp.concatenate((readout[:, 0], -readout[:, 1]), axis=3)
    mixed = jnp.einsum("kgtn,kghn->tgh", state, out_map, precision=lax.Precision.HIGH)
    return mixed.reshape(rows, groups * width) + skip_gain[None, :] * mixer_input.astype(
        jnp.float32
    )


gather_paths = (("z", "y", "x"), ("z", "x", "y")) * 2
sum_paths = (("x", "y", "z"), ("y", "x", "z")) * 4
halves = 2
chip_axes = ("z", "y", "x")


def turned(turn):
    turn = turn - 2.0 * jnp.floor(turn * 0.5)
    quarter = jnp.floor(2.0 * turn + 0.5)
    angle = math.pi * (turn - 0.5 * quarter)
    square = angle * angle
    sin = angle + angle * square * (
        -1.6666654611e-1 + square * (8.3321608736e-3 - 1.9515295891e-4 * square)
    )
    cos = (
        1.0
        - 0.5 * square
        + square
        * square
        * (4.166664568298827e-2 + square * (-1.388731625493765e-3 + 2.443315711809948e-5 * square))
    )
    swap = (quarter == 1.0) | (quarter == 3.0)
    full_cos = jnp.where(swap, sin, cos)
    full_sin = jnp.where(swap, cos, sin)
    full_cos = jnp.where((quarter == 1.0) | (quarter == 2.0), -full_cos, full_cos)
    full_sin = jnp.where((quarter == 2.0) | (quarter == 3.0), -full_sin, full_sin)
    return full_cos, full_sin


def turns_of(step_size, count):
    coarse = jnp.floor(step_size * 1024.0 + 0.5) * (1.0 / 1024.0)
    whole = coarse * count
    whole = whole - 2.0 * jnp.floor(whole * 0.5)
    return whole + (step_size - coarse) * count


def drive_scale(step_size):
    series = 1.0 / 720.0
    for term in (120.0, 24.0, 6.0, 2.0, 1.0):
        series = 1.0 / term - step_size * series
    return jnp.sqrt(
        jnp.where(step_size < 0.25, step_size * series, 1.0 - jnp.exp(-step_size))
    )


def layer_kernel(sizes, *refs):
    (
        x_ref,
        step_ref,
        damping_ref,
        in_ref,
        readout_ref,
        skip_ref,
        gain_ref,
        value_taps_ref,
        gate_taps_ref,
        residual_ref,
        channel_ref,
        out_w_hbm,
        value_hbm,
        gate_hbm,
        down_hbm,
        out_ref,
        x_t,
        decay_parts,
        local,
        carried,
        tab_ref,
        turn_ref,
        totals,
        totals_all,
        ends,
        packet,
        packets,
        carry,
        y_all,
        y_land,
        gain_all,
        out_w,
        state_rows,
        taps,
        up_w,
        down_w,
        held_up,
        held_down,
        rows_all,
        up_rows,
        hidden_rows,
        partial,
    ) = refs[:42]
    sums_in = len(sum_paths)
    landing = refs[42 : 42 + 3 * sums_in]
    (
        local_sem,
        small_send,
        small_recv,
        taps_sem,
        hop_send,
        hop_recv,
        line_send,
        line_recv,
        hold_send,
        hold_recv,
        w_send,
        w_recv,
        f_send,
        f_recv,
    ) = refs[42 + 3 * sums_in :]
    span, channels = x_ref.shape
    groups, head, states = in_ref.shape[2:]
    pairs, heads, lanes = groups // 2, 2 * head, 2 * states
    tiles = span // 8
    pieces = len(gather_paths)
    rows, width = residual_ref.shape
    piece_width = width // pieces
    depth = value_hbm.shape[0]
    part = down_hbm.shape[1]
    sub = part // halves
    unit = taps.shape[2]
    cores = sizes["c"]
    count, tp_count = sizes["z"] * sizes["y"], sizes["x"] * cores
    per = count // cores
    blocks = count * sizes["x"]
    sp, tp = lax.axis_index("sp"), lax.axis_index("tp")
    mine = {
        "z": sp // sizes["y"],
        "y": lax.rem(sp, sizes["y"]),
        "x": tp // cores,
        "c": lax.rem(tp, cores),
    }
    core = mine["c"]
    partner = (sp, mine["x"] * cores + lax.rem(core + 1, cores))

    def neighbour(axis, offset):
        at = dict(mine)
        at[axis] = lax.rem(mine[axis] + offset, sizes[axis])
        return at[axis], (at["z"] * sizes["y"] + at["y"], at["x"] * cores + at["c"])

    def remote(source, target, send, recv, device):
        return pltpu.make_async_remote_copy(
            src_ref=source,
            dst_ref=target,
            send_sem=send,
            recv_sem=recv,
            device_id=device,
            device_id_type=mesh_ids,
        )

    barrier = pltpu.get_barrier_semaphore()
    greeted = 0
    for offset in range(count):
        for turn in range(cores):
            if offset or turn:
                peer = lax.rem(sp + offset, count)
                other = mine["x"] * cores + lax.rem(core + turn, cores)
                pl.semaphore_signal(barrier, inc=1, device_id=(peer, other), device_id_type=mesh_ids)
                greeted += 1
    for offset in range(1, sizes["x"]):
        for turn in range(cores):
            other = lax.rem(mine["x"] + offset, sizes["x"]) * cores + turn
            pl.semaphore_signal(barrier, inc=1, device_id=(sp, other), device_id_type=mesh_ids)
            greeted += 1

    out_copy = pltpu.make_async_copy(out_w_hbm, out_w, local_sem.at[0])
    out_copy.start()
    pl.semaphore_wait(barrier, greeted)

    def block_view(kind, source):
        if kind >= 2:
            return down_w.at[kind - 2, :, pl.ds(pl.multiple_of(source * sub, sub), sub)]
        column = kind * unit
        return up_w.at[pl.ds(pl.multiple_of(source * depth, depth), depth), pl.ds(column, unit)]

    layers = per // sizes["y"]
    across = range(per - layers)
    straight = range(per - layers, per)

    def cut_of(kind, slot, side):
        place = lax.rem(mine["z"] + slot, layers) * sizes["y"] + side
        start = pl.multiple_of(place * unit, unit)
        if kind >= 2:
            source = down_hbm.at[pl.ds(start, unit), pl.ds((kind - 2) * sub, sub)]
        else:
            source = (value_hbm, gate_hbm)[kind].at[:, pl.ds(start, unit)]
        return core * per + place, source

    def weight_copy(kind, slot):
        shift = (slot // layers + 1) % sizes["y"]
        chip, source = cut_of(kind, slot, mine["y"])
        from_y = lax.rem(mine["y"] + sizes["y"] - shift, sizes["y"])
        origin = mine["z"] * sizes["y"] + from_y
        keeper = lax.rem(origin, cores)
        if shift:
            source = (held_down.at[slot, kind - 2] if kind >= 2 else held_up.at[slot, kind])
        stays = (chip == sp) & (keeper == core)
        target = block_view(kind, origin)
        device = (chip, mine["x"] * cores + keeper)

        def here():
            return pltpu.make_async_copy(source, target, w_recv.at[kind, origin // cores])

        def away():
            return remote(source, target, w_send.at[kind, slot], w_recv.at[kind, origin // cores], device)

        return stays, here, away

    def hold_copy(kind, slot):
        side = lax.rem(mine["y"] + slot // layers + 1, sizes["y"])
        _, source = cut_of(kind, slot, side)
        held = held_down.at[slot, kind - 2] if kind >= 2 else held_up.at[slot, kind]
        device = (mine["z"] * sizes["y"] + side, tp)
        return remote(source, held, hold_send.at[kind, slot], hold_recv.at[kind, slot], device)

    def hand_over(kinds, slots):
        for slot in slots:
            for kind in kinds:
                hold_copy(kind, slot).start()

    def send_weights(kinds, slots):
        for slot in slots:
            for kind in kinds:
                if slot in across:
                    hold_copy(kind, slot).wait_recv()
                stays, here, away = weight_copy(kind, slot)
                pl.when(stays)(lambda: here().start())
                pl.when(jnp.logical_not(stays))(lambda: away().start())

    def finish_sends():
        for slot in range(per):
            for kind in range(2 + halves):
                if slot in across:
                    hold_copy(kind, slot).wait_send()
                stays, _, away = weight_copy(kind, slot)
                pl.when(jnp.logical_not(stays))(lambda: away().wait_send())

    def passed_on(kinds, side, index):
        source = side + cores * index
        if kinds[0] >= 2:
            view = block_view(kinds[0], source)
        else:
            view = up_w.at[pl.ds(pl.multiple_of(source * depth, depth), depth), :]
        at = max(kinds[0] - 1, 0)
        return remote(view, view, f_send.at[at, index], f_recv.at[at, index], partner)

    def forward_weights(kinds):
        started = []
        for index in range(per):
            for kind in kinds:
                view = block_view(kind, core + cores * index)
                remote(view, view, w_send.at[kind, 0], w_recv.at[kind, index], partner).wait_recv()
            copy = passed_on(kinds, core, index)
            copy.start()
            started.append(copy)
        return started

    def forwarded(kinds, started):
        for copy in started:
            copy.wait_send()
        for index in range(per):
            passed_on(kinds, lax.rem(core + 1, cores), index).wait_recv()

    hand_over((0,), across[:1])
    send_weights((0,), straight[:1])

    early_copies = []

    sends_at = {"gain": 0, "total": tp_count, "carry": tp_count + count}
    sends_at["y"] = sends_at["edge"] = sends_at["carry"]
    lands_at = dict(sends_at)
    lands_at["y"] = lands_at["carry"] + count
    lands_at["edge"] = lands_at["y"] + tp_count

    def small(source, target, kind, index, device):
        send = small_send.at[sends_at[kind] + index - 1]
        return remote(source, target, send, small_recv.at[lands_at[kind] + index - 1], device)

    for offset in range(1, tp_count):
        peer = (sp, lax.rem(tp + offset, tp_count))
        copy = small(gain_ref, gain_all.at[tp], "gain", offset, peer)
        copy.start()
        early_copies.append(copy)
    gain_all[tp] = gain_ref[...]

    owns_taps = core == sp // per
    taps_start = pl.ds(pl.multiple_of(lax.rem(sp, per) * unit, unit), unit)
    taps_copies = []
    for kind, source in enumerate((value_taps_ref, gate_taps_ref)):
        view = source.at[:, taps_start]
        keep = pltpu.make_async_copy(view, taps.at[kind], taps_sem.at[3 * kind])
        send = remote(
            view, taps.at[kind], taps_sem.at[3 * kind + 1], taps_sem.at[3 * kind + 2], partner
        )
        taps_copies.append((keep, send))

    @pl.when(owns_taps)
    def _():
        for keep, send in taps_copies:
            keep.start()
            send.start()

    pick_group = lax.broadcasted_iota(jnp.int32, (groups, lanes), 0)
    pick_side = lax.broadcasted_iota(jnp.int32, (groups, lanes), 1) // states
    pick_odd = (lax.rem(pick_group, 2) == pick_side).astype(jnp.bfloat16)
    own_pair = lax.broadcasted_iota(
        jnp.int32, (pairs, groups), 1
    ) // 2 == lax.broadcasted_iota(jnp.int32, (pairs, groups), 0)

    def over_lanes(row):
        left = jnp.where(own_pair, jnp.broadcast_to(row, (pairs, groups)), 0.0)
        found = jnp.zeros((pairs, lanes), jnp.float32)
        for _ in range(3):
            rounded = left.astype(jnp.bfloat16)
            found = found + jnp.dot(rounded, pick_odd, preferred_element_type=jnp.float32)
            left = left - rounded.astype(jnp.float32)
        return found

    number = lax.rem(lax.broadcasted_iota(jnp.int32, (8, lanes), 1), states).astype(jnp.float32)
    near = lax.broadcasted_iota(jnp.int32, (8, lanes), 0).astype(jnp.float32)
    for k in range(2):
        step_size = step_ref[k : k + 1, :]
        log_decay = -0.5 * step_size - jnp.transpose(damping_ref[k])
        rows_at = pl.ds(k * pairs, pairs)
        totals[rows_at, :] = over_lanes(jnp.exp(jnp.sum(log_decay, axis=0, keepdims=True)))
        left = jnp.exp(log_decay)
        for level in range(3):
            rounded = left.astype(jnp.bfloat16)
            decay_parts[k, :, level * groups : (level + 1) * groups] = rounded
            left = left - rounded.astype(jnp.float32)
    total_copies = []
    for offset in range(1, count):
        peer = (lax.rem(sp + offset, count), tp)
        copy = small(totals, totals_all.at[sp], "total", offset, peer)
        copy.start()
        total_copies.append(copy)
    totals_all[sp] = totals[...]
    for k in range(2):
        step_size = step_ref[k : k + 1, :]
        rows_at = pl.ds(k * pairs, pairs)
        wide_step = over_lanes(step_size)
        turn_ref[2, rows_at, :] = over_lanes(drive_scale(step_size))
        cos, sin = turned(turns_of(wide_step, number * span))
        turn_ref[0, rows_at, :] = cos
        turn_ref[1, rows_at, :] = sin
        reach = near + 1.0 if k == 0 else 8.0 - near
        for pair in range(pairs):
            cos, sin = turned(turns_of(wide_step[pair : pair + 1], number * reach))
            tab_ref[k * pairs + pair, 0] = cos
            tab_ref[k * pairs + pair, 1] = sin

    x_t[...] = jnp.transpose(x_ref[...].astype(jnp.float32)).astype(jnp.bfloat16)
    row_in_tile = lax.broadcasted_iota(jnp.int32, (1, 8, lanes), 1)
    pick_row = lax.rem(lax.broadcasted_iota(jnp.int32, (3 * groups, lanes), 0), groups)
    pick_lane = lax.broadcasted_iota(jnp.int32, (3 * groups, lanes), 1) // (lanes // 2)

    def both_groups(ref, pair):
        blocks_of = []
        empty = jnp.zeros((head, states), jnp.float32)
        for k in range(2):
            for kind in range(2):
                first = ref[k, kind, 2 * pair].astype(jnp.float32)
                second = ref[k, kind, 2 * pair + 1].astype(jnp.float32)
                upper = jnp.concatenate((first, empty), axis=1)
                lower = jnp.concatenate((empty, second), axis=1)
                blocks_of.append(jnp.concatenate((upper, lower), axis=0))
        return jnp.concatenate(blocks_of, axis=1)

    def chain(k, at, start_real, start_imag):
        real, imag = start_real, start_imag
        found = [None] * tiles
        for tile in range(tiles) if k == 0 else range(tiles - 1, -1, -1):
            place = pl.ds(tile * 8, 8)
            cos, sin = carried[at, 0, place, :], carried[at, 1, place, :]
            full_real = local[at, 0, place, :] + (cos * real - sin * imag)
            full_imag = local[at, 1, place, :] + (cos * imag + sin * real)
            found[tile] = (full_real, full_imag)
            edge = slice(7, 8) if k == 0 else slice(0, 1)
            real = jnp.broadcast_to(full_real[edge], (8, lanes))
            imag = jnp.broadcast_to(full_imag[edge], (8, lanes))
        return found, real, imag

    def first_pass(pair, _):
        inputs = x_t[pl.ds(pl.multiple_of(pair * heads, heads), heads), :]
        driven = lax.dot_general(
            inputs,
            both_groups(in_ref, pair).astype(jnp.bfloat16),
            (((0,), (0,)), ((), ())),
            preferred_element_type=jnp.float32,
        )
        for k in range(2):
            at = k * pairs + pair
            pick = (pick_row == 2 * pair + pick_lane).astype(jnp.bfloat16)
            cover = jnp.dot(decay_parts[k], pick, preferred_element_type=jnp.float32)
            cover = cover.reshape(tiles, 8, lanes)
            base = 2 * k * lanes
            scale = turn_ref[2, pl.ds(at, 1), :]
            real = (driven[:, base : base + lanes] * scale).reshape(tiles, 8, lanes)
            imag = (driven[:, base + lanes : base + 2 * lanes] * scale).reshape(tiles, 8, lanes)
            for reach in (1, 2, 4):
                row = reach - 1 if k == 0 else 8 - reach
                shift = reach if k == 0 else 8 - reach
                valid = row_in_tile >= reach if k == 0 else row_in_tile < 8 - reach
                cos = tab_ref[at, 0, row : row + 1, :].reshape(1, 1, lanes)
                sin = tab_ref[at, 1, row : row + 1, :].reshape(1, 1, lanes)
                moved_real = pltpu.roll(real, shift, 1)
                moved_imag = pltpu.roll(imag, shift, 1)
                decay = jnp.where(valid, cover, 0.0)
                real = real + decay * (cos * moved_real - sin * moved_imag)
                imag = imag + decay * (cos * moved_imag + sin * moved_real)
                cover = cover * jnp.where(valid, pltpu.roll(cover, shift, 1), 1.0)
            local[at, 0] = real.reshape(span, lanes)
            local[at, 1] = imag.reshape(span, lanes)
            carried[at, 0] = (cover * tab_ref[at, 0].reshape(1, 8, lanes)).reshape(span, lanes)
            carried[at, 1] = (cover * tab_ref[at, 1].reshape(1, 8, lanes)).reshape(span, lanes)
        for k in range(2):
            at = k * pairs + pair
            none = jnp.zeros((8, lanes), jnp.float32)
            real, imag = chain(k, at, none, none)[1:]
            ends[pl.ds(at, 1), :] = real[0:1]
            ends[pl.ds(2 * pairs + at, 1), :] = imag[0:1]
        return _

    lax.fori_loop(0, pairs, first_pass, 0)

    packet[...] = ends[...].astype(jnp.bfloat16)
    packets[sp] = packet[...]
    carry_copies = []
    for offset in range(1, count):
        peer = (lax.rem(sp + offset, count), tp)
        copy = small(packet, packets.at[sp], "carry", offset, peer)
        copy.start()
        carry_copies.append(copy)
    for copy in total_copies + carry_copies:
        copy.wait()
    hand_over((1,), across[:1])
    hand_over((0, 1), across[1:])
    send_weights((1,), straight[:1])
    send_weights((0,), straight[1:])

    for k in range(2):
        at = pl.ds(k * pairs, pairs)
        cos, sin = turn_ref[0, at, :], turn_ref[1, at, :]
        real = jnp.zeros((pairs, lanes), jnp.float32)
        imag = real
        for index in range(count) if k == 0 else range(count - 1, -1, -1):
            total = totals_all[index, at, :]
            end = packets[index].astype(jnp.float32)
            end_real = end[k * pairs : (k + 1) * pairs]
            end_imag = end[(2 + k) * pairs : (3 + k) * pairs]
            turned_real = cos * real - sin * imag
            turned_imag = cos * imag + sin * real
            before = (index < sp) if k == 0 else (index > sp)
            real = jnp.where(before, end_real + total * turned_real, real)
            imag = jnp.where(before, end_imag + total * turned_imag, imag)
        carry[0, at, :] = real
        carry[1, at, :] = imag

    gains = skip_ref[...] * x_ref[...].astype(jnp.float32)
    for pair in range(pairs):
        parts = []
        for k in range(2):
            at = k * pairs + pair
            real = jnp.broadcast_to(carry[0, at : at + 1, :], (8, lanes))
            imag = jnp.broadcast_to(carry[1, at : at + 1, :], (8, lanes))
            found, _, _ = chain(k, at, real, imag)
            parts.append(jnp.concatenate([item[0] for item in found], axis=0))
            parts.append(jnp.concatenate([item[1] for item in found], axis=0))
        state = jnp.concatenate(parts, axis=1)
        state_high = state.astype(jnp.bfloat16)
        state_low = (state - state_high.astype(jnp.float32)).astype(jnp.bfloat16)
        sign = jnp.concatenate([jnp.full((1, lanes), v, jnp.float32) for v in (1, -1, 1, -1)], axis=1)
        out_map = both_groups(readout_ref, pair) * sign
        map_high = out_map.astype(jnp.bfloat16)
        map_low = (out_map - map_high.astype(jnp.float32)).astype(jnp.bfloat16)

        def apply(left, right):
            return lax.dot_general(
                left, right, (((1,), (1,)), ((), ())), preferred_element_type=jnp.float32
            )

        both = apply(state_high, jnp.concatenate((map_high, map_low), axis=0))
        mixed = both[:, :heads] + both[:, heads:] + apply(state_low, map_high)
        columns = slice(pair * heads, (pair + 1) * heads)
        y_all[:, columns] = mixed + gains[:, columns]
    y_copies = []
    for offset in range(1, tp_count):
        peer = lax.rem(tp + offset, tp_count)
        part_rows = y_all.at[pl.ds(pl.multiple_of(peer * rows, rows), rows), :]
        copy = small(part_rows, y_land.at[tp], "y", offset, (sp, peer))
        copy.start()
        y_copies.append(copy)
    y_land[tp] = y_all[pl.ds(pl.multiple_of(tp * rows, rows), rows), :]
    for copy in early_copies + y_copies:
        copy.wait()
    out_copy.wait()

    mixed = jnp.concatenate([y_land[peer] for peer in range(tp_count)], axis=1)
    gain = jnp.concatenate([gain_all[peer] for peer in range(tp_count)], axis=1)
    inverse = lax.rsqrt(jnp.mean(mixed * mixed, axis=1, keepdims=True) + norm_eps)
    normed_mix = (mixed * inverse * gain).astype(jnp.bfloat16)
    square = jnp.zeros((rows, 1), jnp.float32)
    tile = 512
    for start in range(0, width, tile):
        columns = pl.ds(start, tile)
        mixed_rows = jnp.dot(normed_mix, out_w[:, columns], preferred_element_type=jnp.float32)
        summed = (residual_ref[:, columns].astype(jnp.float32) + mixed_rows).astype(jnp.bfloat16)
        state_rows[:, columns] = summed
        wide = summed.astype(jnp.float32)
        square = square + jnp.sum(wide * wide, axis=1, keepdims=True)
    scale_rows = lax.rsqrt(square / width + norm_eps)
    normed = state_rows[...].astype(jnp.float32) * scale_rows * channel_ref[...]
    rows_all[mine["z"], mine["y"], mine["x"]] = normed.astype(jnp.bfloat16)

    deep = sizes["z"] // 2
    base = mine["z"] // deep * deep
    other = deep - base
    relays = mine["z"] == deep - 1 + base // deep
    far_end = deep - base // deep

    def plane(z):
        return z * sizes["y"] + mine["y"], tp

    def line_copy(piece, source, target, at):
        columns = pl.ds(piece * piece_width, piece_width)
        view = rows_all.at[source, mine["y"], mine["x"], :, columns]
        return remote(
            view, view, line_send.at[piece, at], line_recv.at[piece, source], plane(target)
        )

    def line_start(piece):
        line_copy(piece, mine["z"], far_end, 0).start()
        for offset in range(1, deep):
            line_copy(piece, mine["z"], base + lax.rem(mine["z"] + offset, deep), offset).start()

    def line_relay(piece, action):
        for index in range(deep):
            for offset in range(1, deep):
                at = deep + index * (deep - 1) + offset - 1
                target = base + lax.rem(mine["z"] + offset, deep)
                copy = line_copy(piece, other + index, target, at)
                copy.start() if action == "start" else copy.wait_send()

    def line_finish(piece):
        for index in range(deep):
            line_copy(piece, other + index, far_end, 0).wait_recv()
        pl.when(relays)(lambda: line_relay(piece, "start"))
        for offset in range(1, deep):
            source = base + lax.rem(mine["z"] + offset, deep)
            line_copy(piece, source, far_end, 0).wait_recv()

    def line_sent(piece):
        for at in range(deep):
            line_copy(piece, mine["z"], far_end, at).wait_send()
        pl.when(relays)(lambda: line_relay(piece, "sent"))

    for piece in range(pieces):
        line_start(piece)

    send_weights((1,), straight[1:])

    slot = 0
    sums_at = pieces * (sizes["y"] + sizes["x"] - 2)
    pending = [[] for _ in range(pieces)]
    for stage in range(1, 3):
        for piece in range(pieces):
            if stage == 1:
                line_finish(piece)
            axis = gather_paths[piece][stage]
            done = gather_paths[piece][:stage]
            for copy in pending[piece]:
                copy.wait()
            pending[piece] = []
            index = tuple(slice(None) if name in done else mine[name] for name in chip_axes)
            block = rows_all.at[index + (slice(None), pl.ds(piece * piece_width, piece_width))]
            for offset in range(1, sizes[axis]):
                _, device = neighbour(axis, offset)
                copy = remote(block, block, hop_send.at[slot], hop_recv.at[slot], device)
                copy.start()
                pending[piece].append(copy)
                slot += 1
        if stage == 1:
            send_weights((0, 1), across)
    for kind in range(2, 2 + halves):
        hand_over((kind,), across)
        send_weights((kind,), straight)
    up_started = forward_weights((0, 1))
    for piece in range(pieces):
        for copy in pending[piece]:
            copy.wait()
    for piece in range(pieces):
        line_sent(piece)
    forwarded((0, 1), up_started)

    @pl.when(core == 0)
    def _():
        up_rows[1, pl.ds(0, 8), :] = jnp.zeros((8, 2 * unit), jnp.float32)

    @pl.when(core == cores - 1)
    def _():
        up_rows[blocks, pl.ds(rows + 8, 8), :] = jnp.zeros((8, 2 * unit), jnp.float32)

    chunk = 256

    def project(n, _):
        columns = pl.ds(pl.multiple_of(n * chunk, chunk), chunk)
        block = rows_all[...].reshape(blocks * rows, width)
        up = jnp.dot(block, up_w[:, columns], preferred_element_type=jnp.float32)
        up = up.astype(jnp.bfloat16).astype(jnp.float32)
        up_rows[pl.ds(1, blocks), pl.ds(8, rows), columns] = up.reshape(blocks, rows, chunk)
        return _

    lax.fori_loop(0, 2 * unit // chunk, project, 0)

    send_weights((2,), across)
    edges = []
    for kind, (take, land, first) in enumerate(((rows, 0, 1 + core), (8, rows + 8, core))):
        edge = up_rows.at[pl.ds(1, blocks), pl.ds(take, 8), :]
        beyond = up_rows.at[pl.ds(first, blocks), pl.ds(land, 8), :]
        copy = small(edge, beyond, "edge", kind + 1, partner)
        copy.start()
        edges.append(copy)

    @pl.when(owns_taps)
    def _():
        for keep, send in taps_copies:
            keep.wait()
            send.wait_send()

    @pl.when(jnp.logical_not(owns_taps))
    def _():
        for _, send in taps_copies:
            send.wait_recv()

    for copy in edges:
        copy.wait()

    def mix(b, _):
        window = up_rows[b + 1]

        def conv(kind, columns):
            return (
                taps[kind, 0:1, :] * window[7 : rows + 7, columns]
                + taps[kind, 1:2, :] * window[8 : rows + 8, columns]
                + taps[kind, 2:3, :] * window[9 : rows + 9, columns]
            )

        value = conv(0, slice(0, unit))
        gate = conv(1, slice(unit, 2 * unit))
        hidden = value * (gate / (1.0 + jnp.exp(-gate)))
        hidden_rows[pl.ds(pl.multiple_of(b * rows, rows), rows), :] = hidden.astype(jnp.bfloat16)
        return _

    lax.fori_loop(0, blocks, mix, 0)

    for kind in range(3, 2 + halves):
        send_weights((kind,), across)
    sum_width = width // sums_in
    per_half = sums_in // halves

    def start_sum(piece, stage, slot):
        axis = sum_paths[piece][stage]
        done = sum_paths[piece][:stage]
        started = []
        for offset in range(1, sizes[axis]):
            place, device = neighbour(axis, offset)
            index = tuple(
                place if name == axis else mine[name] if name in done else slice(None)
                for name in chip_axes
            )
            copy = remote(
                partial.at[index + (slice(None), pl.ds(piece * sum_width, sum_width))],
                landing[piece * 3 + stage].at[offset - 1],
                hop_send.at[slot],
                hop_recv.at[slot],
                device,
            )
            copy.start()
            started.append(copy)
            slot += 1
        return started, slot

    def add_landed(piece, stage):
        axis = sum_paths[piece][stage]
        done = sum_paths[piece][: stage + 1]
        land = landing[piece * 3 + stage]
        columns = pl.ds(piece * sum_width, sum_width)
        free = [name for name in chip_axes if name not in done]

        def add(step, _):
            index, inner = [], ()
            for name in chip_axes:
                if name in done:
                    index.append(mine[name])
                elif name == free[0]:
                    index.append(step)
                    inner = (step,)
                else:
                    index.append(slice(None))
            index = tuple(index) + (slice(None), columns)
            value = partial[index].astype(jnp.float32)
            for offset in range(1, sizes[axis]):
                value = value + land[(offset - 1,) + inner].astype(jnp.float32)
            if free:
                partial[index] = value.astype(jnp.bfloat16)
            else:
                for step_at in range(sum_width // sub):
                    place = piece % per_half * sum_width // sub + step_at
                    real = pl.ds(place * part + piece // per_half * sub, sub)
                    added = value[:, step_at * sub : (step_at + 1) * sub]
                    out_ref[:, real] = (
                        state_rows[:, real].astype(jnp.float32) + added
                    ).astype(jnp.bfloat16)
            return _

        if free:
            lax.fori_loop(0, sizes[free[0]], add, 0)
        else:
            add(0, 0)

    slot = sums_at
    waiting = {}

    def advance(group, stage, slot):
        for piece in range(group * per_half, (group + 1) * per_half):
            if stage == 0:
                columns = pl.ds(piece % per_half * sum_width, sum_width)
                sums = jnp.dot(
                    hidden_rows[...],
                    down_w[group, :, columns],
                    preferred_element_type=jnp.float32,
                )
                shape = partial.shape[:3] + (rows, sum_width)
                partial[:, :, :, :, pl.ds(piece * sum_width, sum_width)] = sums.astype(
                    jnp.bfloat16
                ).reshape(shape)
            else:
                for copy in waiting[piece]:
                    copy.wait()
                add_landed(piece, stage - 1)
            if stage < 3:
                waiting[piece], slot = start_sum(piece, stage, slot)
        return slot

    down_started = forward_weights((2,))
    for group in range(halves):
        forwarded((2 + group,), down_started)
        slot = advance(group, 0, slot)
        if group + 1 < halves:
            down_started = forward_weights((3 + group,))
        if group:
            slot = advance(group - 1, 2, slot)
        slot = advance(group, 1, slot)
        if group:
            advance(group - 1, 3, slot)
    slot = advance(halves - 1, 2, slot)
    advance(halves - 1, 3, slot)
    finish_sends()


def whole_layer(sizes, arrays, weights, unit):
    x, time_step, _, in_map, _, _, gain, value_taps, _, residual, _ = arrays
    out_weight, value_weight, gate_weight, down_weight = weights
    span, channels = x.shape
    groups, lanes = time_step.shape[1], 2 * in_map.shape[4]
    chains = groups
    rows, width = residual.shape
    pieces, sums_in = len(gather_paths), len(sum_paths)
    count, tp_count = sizes["z"] * sizes["y"], sizes["x"] * sizes["c"]
    grid = tuple(sizes[name] for name in chip_axes)
    blocks = math.prod(grid)
    per = count // sizes["c"]
    landing = []
    for order in sum_paths:
        for stage in range(3):
            axis = order[stage]
            left = tuple(sizes[name] for name in chip_axes if name not in order[: stage + 1])
            landing.append(
                pltpu.VMEM((max(sizes[axis] - 1, 1),) + left + (rows, width // sums_in), jnp.bfloat16)
            )
    gather_hops = pieces * (sizes["y"] + sizes["x"] - 2)
    sum_hops = sums_in * sum(sizes[name] - 1 for name in chip_axes)
    deep = sizes["z"] // 2
    aside = max(per - per // sizes["y"], 1)
    vmem = pl.BlockSpec(memory_space=pltpu.VMEM)
    far = pl.BlockSpec(memory_space=pl.ANY)
    dma = pltpu.SemaphoreType.DMA
    f32, bf16 = jnp.float32, jnp.bfloat16
    return pl.pallas_call(
        lambda *refs: layer_kernel(sizes, *refs),
        name="whole_layer",
        out_shape=jax.ShapeDtypeStruct((rows, width), bf16),
        in_specs=[vmem] * 11 + [far] * 4,
        out_specs=vmem,
        scratch_shapes=[
            pltpu.VMEM((channels, span), bf16),
            pltpu.VMEM((2, span, 3 * groups), bf16),
            pltpu.VMEM((chains, 2, span, lanes), f32),
            pltpu.VMEM((chains, 2, span, lanes), f32),
            pltpu.VMEM((chains, 2, 8, lanes), f32),
            pltpu.VMEM((3, chains, lanes), f32),
            pltpu.VMEM((chains, lanes), f32),
            pltpu.VMEM((count, chains, lanes), f32),
            pltpu.VMEM((2 * chains, lanes), f32),
            pltpu.VMEM((2 * chains, lanes), bf16),
            pltpu.VMEM((count, 2 * chains, lanes), bf16),
            pltpu.VMEM((2, chains, lanes), f32),
            pltpu.VMEM((span, channels), f32),
            pltpu.VMEM((tp_count, rows, channels), f32),
            pltpu.VMEM((tp_count,) + gain.shape, f32),
            pltpu.VMEM(out_weight.shape, bf16),
            pltpu.VMEM((rows, width), bf16),
            pltpu.VMEM((2, value_taps.shape[0], unit), f32),
            pltpu.VMEM((width, 2 * unit), bf16),
            pltpu.VMEM((halves, unit, width // halves), bf16),
            pltpu.VMEM((aside, 2, width // count, unit), bf16),
            pltpu.VMEM((aside, halves, unit, width // count // halves), bf16),
            pltpu.VMEM(grid + (rows, width), bf16),
            pltpu.VMEM((blocks + 2, rows + 16, 2 * unit), f32),
            pltpu.VMEM((blocks * rows, unit), bf16),
            pltpu.VMEM(grid + (rows, width), bf16),
            *landing,
            dma((1,)),
            dma((tp_count + 2 * count + 2,)),
            dma((2 * tp_count + 2 * count + 2,)),
            dma((6,)),
            dma((gather_hops + sum_hops,)),
            dma((gather_hops + sum_hops,)),
            dma((pieces, deep * deep)),
            dma((pieces, sizes["z"])),
            dma((2 + halves, aside)),
            dma((2 + halves, aside)),
            dma((2 + halves, per)),
            dma((2 + halves, per)),
            dma((1 + halves, per)),
            dma((1 + halves, per)),
        ],
        compiler_params=pltpu.CompilerParams(
            collective_id=2, has_side_effects=True, vmem_limit_bytes=63 * 1024 * 1024
        ),
    )(*arrays, *weights)


def mesh_sizes(sp_count, tp_count):
    cores = 2
    across = tp_count // cores
    deep = math.gcd(across, sp_count)
    return {"z": sp_count // deep, "y": deep, "x": across, "c": cores}


def tile_units(sizes, x_shape, in_shape, value_shape, down_shape, residual_shape):
    count = sizes["z"] * sizes["y"]
    unit = value_shape[1] * sizes["c"] // count
    rows, width = residual_shape
    span, states, head = x_shape[0], in_shape[3], in_shape[4]
    fits = (
        sizes["z"] % 2 == 0
        and sizes["z"] % sizes["c"] == 0
        and unit % 128 == 0
        and 2 * unit % 256 == 0
        and value_shape[0] % 16 == 0
        and down_shape[1] % (128 * halves) == 0
        and width // len(sum_paths) % (down_shape[1] // halves) == 0
        and width % 512 == 0
        and rows % 16 == 0
        and span % 128 == 0
        and 2 * states == 128
        and in_shape[2] % 16 == 0
        and width % (256 * len(gather_paths)) == 0
        and head % 16 == 0
        and x_shape[1] % 128 == 0
    )
    return unit if fits else 0


def one_kernel(sizes, unit, args):
    (
        mixer_input,
        time_step,
        damping,
        input_map,
        readout,
        skip_gain,
        out_gain,
        out_weight,
        residual,
        channel_gain,
        value_weight,
        gate_weight,
        value_taps,
        gate_taps,
        down_weight,
    ) = args
    arrays = (
        mixer_input,
        time_step,
        damping.swapaxes(1, 2),
        input_map.swapaxes(3, 4),
        readout,
        skip_gain.reshape(1, -1),
        out_gain.reshape(1, -1),
        value_taps,
        gate_taps,
        residual,
        channel_gain.reshape(1, -1),
    )
    return whole_layer(
        sizes, arrays, (out_weight, value_weight, gate_weight, down_weight), unit
    )


def body(
    mixer_input,
    time_step,
    damping,
    input_map,
    readout,
    skip_gain,
    out_gain,
    out_weight,
    residual,
    channel_gain,
    value_weight,
    gate_weight,
    value_taps,
    gate_taps,
    down_weight,
):
    count, mine = lax.axis_size("sp"), lax.axis_index("sp")
    sizes = mesh_sizes(count, lax.axis_size("tp"))
    unit = tile_units(
        sizes,
        mixer_input.shape,
        input_map.shape,
        value_weight.shape,
        down_weight.shape,
        residual.shape,
    )
    if unit:
        args = (mixer_input, time_step, damping, input_map, readout, skip_gain, out_gain)
        args += (out_weight, residual, channel_gain, value_weight, gate_weight)
        return one_kernel(sizes, unit, args + (value_taps, gate_taps, down_weight))
    depth, hidden_width = value_weight.shape
    part = hidden_width // count
    up_send = jnp.concatenate(
        (
            value_weight.reshape(depth, count, part).swapaxes(0, 1),
            gate_weight.reshape(depth, count, part).swapaxes(0, 1),
        ),
        axis=2,
    )
    down_send = down_weight.reshape(count, part, down_weight.shape[1])
    mixed_y = mixer(mixer_input, time_step, damping, input_map, readout, skip_gain)
    tp_count = lax.axis_size("tp")
    mixed_y = mixed_y.reshape(tp_count, -1, out_gain.shape[0])
    gain_row = jnp.broadcast_to(out_gain, (tp_count, 1, out_gain.shape[0]))
    mixed_y = jnp.concatenate((mixed_y, gain_row), axis=1)
    mixed_y = lax.all_to_all(mixed_y, "tp", split_axis=0, concat_axis=0, tiled=True)
    mixed_y = mixed_y.swapaxes(0, 1).reshape(mixed_y.shape[1], -1)
    mixed_y, gain = mixed_y[:-1], mixed_y[-1]
    inverse = lax.rsqrt(jnp.mean(mixed_y * mixed_y, axis=1, keepdims=True) + norm_eps)
    normed_mix = (mixed_y * inverse * gain[None, :]).astype(jnp.bfloat16)
    mixed_rows = jnp.dot(normed_mix, out_weight, preferred_element_type=jnp.float32)
    hidden_state = (residual.astype(jnp.float32) + mixed_rows).astype(jnp.bfloat16)
    state_wide = hidden_state.astype(jnp.float32)
    scale_rows = lax.rsqrt(jnp.mean(state_wide * state_wide, axis=1, keepdims=True) + norm_eps)
    normed = (state_wide * scale_rows * channel_gain[None, :]).astype(jnp.bfloat16)
    taps = jnp.concatenate(
        (
            lax.dynamic_slice_in_dim(value_taps, mine * part, part, axis=1),
            lax.dynamic_slice_in_dim(gate_taps, mine * part, part, axis=1),
        ),
        axis=1,
    )
    return channel_mixer(normed, hidden_state, up_send, down_send, taps, count, tp_count)


def solution(mesh):
    in_specs = (
        P("sp", "tp"),
        P(None, "tp"),
        P(None, "sp", "tp"),
        P(None, None, "tp", None, None),
        P(None, None, "tp", None, None),
        P("tp"),
        P("tp"),
        P(),
        P(("sp", "tp"), None),
        P(),
        P("sp", "tp"),
        P("sp", "tp"),
        P(None, "tp"),
        P(None, "tp"),
        P("tp", "sp"),
    )
    out_specs = P(("sp", "tp"), None)
    return jax.shard_map(body, mesh=mesh, in_specs=in_specs, out_specs=out_specs, check_vma=False)
```

```python
import math

import jax
import jax.numpy as jnp
from jax import lax
from jax.experimental import pallas as pl
from jax.experimental.pallas import tpu as pltpu
from jax.sharding import PartitionSpec as P

norm_eps = 1e-06
highest = lax.Precision.HIGHEST
mesh_ids = pl.DeviceIdType.MESH


def carry_kernel(count, own_ref, all_ref, local_sem, send_sem, recv_sem):
    sp, tp = lax.axis_index("sp"), lax.axis_index("tp")
    barrier = pltpu.get_barrier_semaphore()
    for offset in range(1, count):
        peer = lax.rem(sp + offset, count)
        pl.semaphore_signal(barrier, inc=1, device_id=(peer, tp), device_id_type=mesh_ids)
    pl.semaphore_wait(barrier, count - 1)
    keep = pltpu.make_async_copy(own_ref, all_ref.at[sp], local_sem)
    keep.start()
    copies = []
    for offset in range(1, count):
        peer = lax.rem(sp + offset, count)
        copy = pltpu.make_async_remote_copy(
            src_ref=own_ref,
            dst_ref=all_ref.at[sp],
            send_sem=send_sem.at[offset],
            recv_sem=recv_sem.at[offset],
            device_id=(peer, tp),
            device_id_type=mesh_ids,
        )
        copy.start()
        copies.append(copy)
    keep.wait()
    for copy in copies:
        copy.wait()


def gather_ends(packed, count):
    vmem = pl.BlockSpec(memory_space=pltpu.VMEM)
    return pl.pallas_call(
        lambda *refs: carry_kernel(count, *refs),
        name="gather_ends",
        out_shape=jax.ShapeDtypeStruct((count,) + packed.shape, packed.dtype),
        in_specs=[vmem],
        out_specs=vmem,
        scratch_shapes=[
            pltpu.SemaphoreType.DMA,
            pltpu.SemaphoreType.DMA((count,)),
            pltpu.SemaphoreType.DMA((count,)),
        ],
        compiler_params=pltpu.CompilerParams(collective_id=0, has_side_effects=True),
    )(packed)


gather_orders = (("z", "y", "x", "c"), ("y", "z", "x", "c"))
sum_orders = (("c", "x", "y", "z"), ("c", "z", "y", "x"))
axes = ("z", "y", "x", "c")


def channel_kernel(sizes, *refs):
    normed_ref, hidden_state_ref, up_send, down_send, taps_ref, out_ref = refs[:6]
    rows_all, up_rows, partial, up_land, down_land, down_ref = refs[6:12]
    landing = refs[12:20]
    local_sem, send_sem, recv_sem, weight_send_sem, weight_recv_sem = refs[20:25]
    rows, width = normed_ref.shape
    half = width // 2
    count, part, part_width = down_send.shape
    sp, tp = lax.axis_index("sp"), lax.axis_index("tp")
    mine = {
        "z": sp // sizes["y"],
        "y": lax.rem(sp, sizes["y"]),
        "x": tp // sizes["c"],
        "c": lax.rem(tp, sizes["c"]),
    }

    def neighbour(axis, offset):
        at = dict(mine)
        at[axis] = lax.rem(mine[axis] + offset, sizes[axis])
        return at[axis], (at["z"] * sizes["y"] + at["y"], at["x"] * sizes["c"] + at["c"])

    barrier = pltpu.get_barrier_semaphore()
    greeted = 0
    for axis in ("x", "c"):
        for offset in range(1, sizes[axis]):
            _, device = neighbour(axis, offset)
            pl.semaphore_signal(barrier, inc=1, device_id=device, device_id_type=mesh_ids)
            greeted += 1
    for offset in range(1, count):
        peer = lax.rem(sp + offset, count)
        pl.semaphore_signal(barrier, inc=1, device_id=(peer, tp), device_id_type=mesh_ids)
        greeted += 1
    pl.semaphore_wait(barrier, greeted)

    keeps = []
    for kind, (source, target) in enumerate(
        (
            (normed_ref, rows_all.at[mine["z"], mine["y"], mine["x"], mine["c"]]),
            (up_send.at[sp], up_land.at[sp]),
            (down_send.at[sp], down_land.at[sp]),
        )
    ):
        keep = pltpu.make_async_copy(source, target, local_sem.at[kind])
        keep.start()
        keeps.append(keep)
    keeps[0].wait()

    def spread(source, land, kind):
        started = []
        for offset in range(1, count):
            peer = lax.rem(sp + offset, count)
            copy = pltpu.make_async_remote_copy(
                src_ref=source.at[peer],
                dst_ref=land.at[sp],
                send_sem=weight_send_sem.at[kind, offset],
                recv_sem=weight_recv_sem.at[kind, offset],
                device_id=(peer, tp),
                device_id_type=mesh_ids,
            )
            copy.start()
            started.append(copy)
        return started

    slot = 0
    pending = [[], []]
    up_copies, down_copies = [], []
    for stage in range(4):
        if stage == 2:
            up_copies = spread(up_send, up_land, 0)
            down_copies = spread(down_send, down_land, 1)
        for piece in range(2):
            axis = gather_orders[piece][stage]
            done = gather_orders[piece][:stage]
            for copy in pending[piece]:
                copy.wait()
            pending[piece] = []
            index = tuple(slice(None) if name in done else mine[name] for name in axes)
            block = rows_all.at[index + (slice(None), pl.ds(piece * half, half))]
            for offset in range(1, sizes[axis]):
                _, device = neighbour(axis, offset)
                copy = pltpu.make_async_remote_copy(
                    src_ref=block,
                    dst_ref=block,
                    send_sem=send_sem.at[slot],
                    recv_sem=recv_sem.at[slot],
                    device_id=device,
                    device_id_type=mesh_ids,
                )
                copy.start()
                pending[piece].append(copy)
                slot += 1
    for piece in range(2):
        for copy in pending[piece]:
            copy.wait()

    plane = sizes["y"] * sizes["x"] * sizes["c"] * rows
    total = plane * sizes["z"]
    for copy in [keeps[1]] + up_copies:
        copy.wait()
    edge = jnp.zeros((8, up_rows.shape[1]), jnp.float32)
    up_rows[pl.ds(0, 8), :] = edge
    up_rows[pl.ds(total + 8, 8), :] = edge

    def project(z, _):
        block = rows_all[z].reshape(plane, width)
        up_weight = up_land[...].reshape(width, 2 * part)
        up = jnp.dot(block, up_weight, preferred_element_type=jnp.float32)
        start = pl.multiple_of(z * plane + 8, 8)
        up_rows[pl.ds(start, plane), :] = up.astype(jnp.bfloat16).astype(jnp.float32)
        return _

    lax.fori_loop(0, sizes["z"], project, 0)

    for copy in [keeps[2]] + down_copies:
        copy.wait()
    for source in range(count):
        down_ref[:, source * part_width : (source + 1) * part_width] = down_land[source]

    def mix(z, _):
        start = pl.multiple_of(z * plane, 8)
        window = up_rows[pl.ds(start, plane + 16), :]
        convolved = (
            taps_ref[0:1, :] * window[7 : plane + 7]
            + taps_ref[1:2, :] * window[8 : plane + 8]
            + taps_ref[2:3, :] * window[9 : plane + 9]
        )
        gate = convolved[:, part:]
        hidden = convolved[:, :part] * (gate / (1.0 + jnp.exp(-gate)))
        sums = jnp.dot(
            hidden.astype(jnp.bfloat16), down_ref[...], preferred_element_type=jnp.float32
        )
        partial[z] = sums.astype(jnp.bfloat16).reshape(partial.shape[1:])
        return _

    lax.fori_loop(0, sizes["z"], mix, 0)

    def start_sum(piece, stage, slot):
        axis = sum_orders[piece][stage]
        done = sum_orders[piece][:stage]
        started = []
        for offset in range(1, sizes[axis]):
            place, device = neighbour(axis, offset)
            index = tuple(
                place if name == axis else mine[name] if name in done else slice(None)
                for name in axes
            )
            copy = pltpu.make_async_remote_copy(
                src_ref=partial.at[index + (slice(None), pl.ds(piece * half, half))],
                dst_ref=landing[piece * 4 + stage].at[offset - 1],
                send_sem=send_sem.at[slot],
                recv_sem=recv_sem.at[slot],
                device_id=device,
                device_id_type=mesh_ids,
            )
            copy.start()
            started.append(copy)
            slot += 1
        return started, slot

    def add_landed(piece, stage):
        axis = sum_orders[piece][stage]
        done = sum_orders[piece][: stage + 1]
        land = landing[piece * 4 + stage]
        columns = pl.ds(piece * half, half)
        free = [name for name in axes if name not in done]

        def add(step, _):
            index, inner = [], ()
            for name in axes:
                if name in done:
                    index.append(mine[name])
                elif name == free[0]:
                    index.append(step)
                    inner = (step,)
                else:
                    index.append(slice(None))
            index = tuple(index) + (slice(None), columns)
            value = partial[index].astype(jnp.float32)
            for offset in range(1, sizes[axis]):
                value = value + land[(offset - 1,) + inner].astype(jnp.float32)
            if free:
                partial[index] = value.astype(jnp.bfloat16)
            else:
                out_ref[:, columns] = (
                    hidden_state_ref[:, columns].astype(jnp.float32) + value
                ).astype(jnp.bfloat16)
            return _

        if free:
            lax.fori_loop(0, sizes[free[0]], add, 0)
        else:
            add(0, 0)

    slot = send_sem.shape[0] // 2
    for stage in range(4):
        for piece in range(2):
            if stage:
                for copy in pending[piece]:
                    copy.wait()
                add_landed(piece, stage - 1)
            pending[piece], slot = start_sum(piece, stage, slot)
    for piece in range(2):
        for copy in pending[piece]:
            copy.wait()
        add_landed(piece, 3)


def channel_mixer(normed, hidden_state, up_send, down_send, taps, sp_count, tp_count):
    cores = 2
    across = tp_count // cores
    deep = math.gcd(across, sp_count)
    sizes = {"z": sp_count // deep, "y": deep, "x": across, "c": cores}
    rows, width = normed.shape
    half = width // 2
    grid = tuple(sizes[name] for name in axes)
    total = math.prod(grid) * rows
    landing = []
    for order in sum_orders:
        for stage in range(4):
            axis = order[stage]
            left = tuple(sizes[name] for name in axes if name not in order[: stage + 1])
            landing.append(
                pltpu.VMEM((max(sizes[axis] - 1, 1),) + left + (rows, half), jnp.bfloat16)
            )
    copies = 2 * 2 * sum(max(sizes[name] - 1, 0) for name in axes)
    vmem = pl.BlockSpec(memory_space=pltpu.VMEM)
    return pl.pallas_call(
        lambda *refs: channel_kernel(sizes, *refs),
        name="channel_mixer",
        out_shape=jax.ShapeDtypeStruct((rows, width), jnp.bfloat16),
        in_specs=[vmem] * 5,
        out_specs=vmem,
        scratch_shapes=[
            pltpu.VMEM(grid + (rows, width), jnp.bfloat16),
            pltpu.VMEM((total + 16, up_send.shape[2]), jnp.float32),
            pltpu.VMEM(grid + (rows, width), jnp.bfloat16),
            pltpu.VMEM(up_send.shape, jnp.bfloat16),
            pltpu.VMEM(down_send.shape, jnp.bfloat16),
            pltpu.VMEM((down_send.shape[1], width), jnp.bfloat16),
            *landing,
            pltpu.SemaphoreType.DMA((3,)),
            pltpu.SemaphoreType.DMA((copies,)),
            pltpu.SemaphoreType.DMA((copies,)),
            pltpu.SemaphoreType.DMA((2, sp_count)),
            pltpu.SemaphoreType.DMA((2, sp_count)),
        ],
        compiler_params=pltpu.CompilerParams(
            collective_id=1, has_side_effects=True, vmem_limit_bytes=63 * 1024 * 1024
        ),
    )(normed, hidden_state, up_send, down_send, taps)


def turns(step_size, count):
    coarse = jnp.round(step_size * 1024.0) / 1024.0
    whole = coarse * count
    whole = whole - 2.0 * jnp.floor(whole * 0.5)
    return whole + (step_size - coarse) * count


def mixer(mixer_input, time_step, damping, input_map, readout, skip_gain):
    rows = mixer_input.shape[0]
    groups = time_step.shape[1]
    states, width = input_map.shape[3], input_map.shape[4]
    count, mine = lax.axis_size("sp"), lax.axis_index("sp")
    at = jnp.arange(rows)
    lower = at[:, None] >= at[None, :]
    reach = jnp.stack((lower, lower.T))
    log_decay = -0.5 * time_step[:, None, :] - damping
    log_sum = jnp.einsum("ktu,kug->kgt", reach.astype(jnp.float32), log_decay, precision=highest)
    weights = jnp.where(
        reach[:, None],
        jnp.exp(jnp.minimum(log_sum[:, :, :, None] - log_sum[:, :, None, :], 0.0)),
        0.0,
    )
    number = jnp.arange(states, dtype=jnp.float32)
    dt = time_step[:, :, None, None]
    angle = math.pi * turns(dt, number[None, :] * at.astype(jnp.float32)[:, None])
    sign = jnp.array([1.0, -1.0], jnp.float32)[:, None, None, None]
    cos, sin = jnp.cos(angle), jnp.sin(angle) * sign
    grouped = mixer_input.reshape(rows, groups, width)
    drive = jnp.einsum("tgh,kpgnh->kpgtn", grouped, input_map, preferred_element_type=jnp.float32)
    drive = drive * jnp.sqrt(-jnp.expm1(-time_step))[:, None, :, None, None]
    rotated = jnp.concatenate(
        (cos * drive[:, 0] + sin * drive[:, 1], cos * drive[:, 1] - sin * drive[:, 0]), axis=3
    )
    local = jnp.einsum("kgts,kgsn->kgtn", weights, rotated, precision=lax.Precision.HIGH)
    ends = jnp.stack((local[0, :, -1], local[1, :, 0]))
    totals = jnp.stack((log_sum[0, :, -1], log_sum[1, :, 0]))
    flat = ends.reshape(2 * groups, 2 * states)
    spare = jnp.pad(totals.reshape(1, 2 * groups), ((0, 7), (0, 2 * states - 2 * groups)))
    every = gather_ends(jnp.concatenate((flat, spare), axis=0), count)
    end_all = every[:, : 2 * groups].reshape(count, 2, groups, 2 * states)
    total_all = every[:, 2 * groups, : 2 * groups].reshape(count, 2, groups)
    index = jnp.arange(count)
    away = jnp.stack((mine - index, index - mine), axis=1)
    lo = jnp.minimum(index, mine)[:, None]
    hi = jnp.maximum(index, mine)[:, None]
    between = ((index[None, :] > lo) & (index[None, :] < hi)).astype(jnp.float32)
    span = jnp.einsum("ji,ikg->jkg", between, total_all, precision=highest)
    factor = jnp.where(away[:, :, None] > 0, jnp.exp(span), 0.0)
    block_turn = turns(time_step[:, :, None], number * rows)
    hop = jnp.abs(mine - index).astype(jnp.float32)[:, None, None, None] * block_turn
    hop = math.pi * (hop - 2.0 * jnp.floor(hop * 0.5))
    hop_cos, hop_sin = jnp.cos(hop) * factor[..., None], jnp.sin(hop) * factor[..., None]
    end_re, end_im = end_all[..., :states], end_all[..., states:]
    carry = jnp.concatenate(
        (
            jnp.sum(hop_cos * end_re - hop_sin * end_im, axis=0),
            jnp.sum(hop_cos * end_im + hop_sin * end_re, axis=0),
        ),
        axis=2,
    )
    local = local + jnp.exp(log_sum)[..., None] * carry[:, :, None, :]
    re, im = local[..., :states], local[..., states:]
    state = jnp.concatenate((cos * re - sin * im, cos * im + sin * re), axis=3)
    out_map = jnp.concatenate((readout[:, 0], -readout[:, 1]), axis=3)
    mixed = jnp.einsum("kgtn,kghn->tgh", state, out_map, precision=lax.Precision.HIGH)
    return mixed.reshape(rows, groups * width) + skip_gain[None, :] * mixer_input.astype(
        jnp.float32
    )


gather_paths = (("z", "y", "x"), ("z", "x", "y")) * 2
sum_paths = (("x", "y", "z"), ("y", "x", "z")) * 4
halves = 2
chip_axes = ("z", "y", "x")


def turned(turn):
    turn = turn - 2.0 * jnp.floor(turn * 0.5)
    quarter = jnp.floor(2.0 * turn + 0.5)
    angle = math.pi * (turn - 0.5 * quarter)
    square = angle * angle
    sin = angle + angle * square * (
        -1.6666654611e-1 + square * (8.3321608736e-3 - 1.9515295891e-4 * square)
    )
    cos = (
        1.0
        - 0.5 * square
        + square
        * square
        * (4.166664568298827e-2 + square * (-1.388731625493765e-3 + 2.443315711809948e-5 * square))
    )
    swap = (quarter == 1.0) | (quarter == 3.0)
    full_cos = jnp.where(swap, sin, cos)
    full_sin = jnp.where(swap, cos, sin)
    full_cos = jnp.where((quarter == 1.0) | (quarter == 2.0), -full_cos, full_cos)
    full_sin = jnp.where((quarter == 2.0) | (quarter == 3.0), -full_sin, full_sin)
    return full_cos, full_sin


def turns_of(step_size, count):
    coarse = jnp.floor(step_size * 1024.0 + 0.5) * (1.0 / 1024.0)
    whole = coarse * count
    whole = whole - 2.0 * jnp.floor(whole * 0.5)
    return whole + (step_size - coarse) * count


def drive_scale(step_size):
    series = 1.0 / 720.0
    for term in (120.0, 24.0, 6.0, 2.0, 1.0):
        series = 1.0 / term - step_size * series
    return jnp.sqrt(
        jnp.where(step_size < 0.25, step_size * series, 1.0 - jnp.exp(-step_size))
    )


def layer_kernel(sizes, *refs):
    (
        x_ref,
        step_ref,
        damping_ref,
        in_ref,
        readout_ref,
        skip_ref,
        gain_ref,
        value_taps_ref,
        gate_taps_ref,
        residual_ref,
        channel_ref,
        out_w_hbm,
        value_hbm,
        gate_hbm,
        down_hbm,
        out_ref,
        x_t,
        decay_parts,
        local,
        carried,
        tab_ref,
        turn_ref,
        totals,
        totals_all,
        ends,
        packet,
        packets,
        carry,
        y_all,
        y_land,
        gain_all,
        out_w,
        state_rows,
        taps,
        up_w,
        down_w,
        held_up,
        held_down,
        rows_all,
        up_rows,
        hidden_rows,
        partial,
    ) = refs[:42]
    sums_in = len(sum_paths)
    landing = refs[42 : 42 + 3 * sums_in]
    (
        local_sem,
        small_send,
        small_recv,
        taps_sem,
        hop_send,
        hop_recv,
        line_send,
        line_recv,
        hold_send,
        hold_recv,
        w_send,
        w_recv,
        f_send,
        f_recv,
    ) = refs[42 + 3 * sums_in :]
    span, channels = x_ref.shape
    groups, head, states = in_ref.shape[2:]
    pairs, heads, lanes = groups // 2, 2 * head, 2 * states
    tiles = span // 8
    pieces = len(gather_paths)
    rows, width = residual_ref.shape
    piece_width = width // pieces
    depth = value_hbm.shape[0]
    part = down_hbm.shape[1]
    sub = part // halves
    unit = taps.shape[2]
    cores = sizes["c"]
    count, tp_count = sizes["z"] * sizes["y"], sizes["x"] * cores
    per = count // cores
    blocks = count * sizes["x"]
    sp, tp = lax.axis_index("sp"), lax.axis_index("tp")
    mine = {
        "z": sp // sizes["y"],
        "y": lax.rem(sp, sizes["y"]),
        "x": tp // cores,
        "c": lax.rem(tp, cores),
    }
    core = mine["c"]
    partner = (sp, mine["x"] * cores + lax.rem(core + 1, cores))

    def neighbour(axis, offset):
        at = dict(mine)
        at[axis] = lax.rem(mine[axis] + offset, sizes[axis])
        return at[axis], (at["z"] * sizes["y"] + at["y"], at["x"] * cores + at["c"])

    def remote(source, target, send, recv, device):
        return pltpu.make_async_remote_copy(
            src_ref=source,
            dst_ref=target,
            send_sem=send,
            recv_sem=recv,
            device_id=device,
            device_id_type=mesh_ids,
        )

    barrier = pltpu.get_barrier_semaphore()
    greeted = 0
    for offset in range(count):
        for turn in range(cores):
            if offset or turn:
                peer = lax.rem(sp + offset, count)
                other = mine["x"] * cores + lax.rem(core + turn, cores)
                pl.semaphore_signal(barrier, inc=1, device_id=(peer, other), device_id_type=mesh_ids)
                greeted += 1
    for offset in range(1, sizes["x"]):
        for turn in range(cores):
            other = lax.rem(mine["x"] + offset, sizes["x"]) * cores + turn
            pl.semaphore_signal(barrier, inc=1, device_id=(sp, other), device_id_type=mesh_ids)
            greeted += 1

    out_copy = pltpu.make_async_copy(out_w_hbm, out_w, local_sem.at[0])
    out_copy.start()
    pl.semaphore_wait(barrier, greeted)

    def block_view(kind, source):
        if kind >= 2:
            return down_w.at[kind - 2, :, pl.ds(pl.multiple_of(source * sub, sub), sub)]
        column = kind * unit
        return up_w.at[pl.ds(pl.multiple_of(source * depth, depth), depth), pl.ds(column, unit)]

    layers = per // sizes["y"]
    across = range(per - layers)
    straight = range(per - layers, per)

    def cut_of(kind, slot, side):
        place = lax.rem(mine["z"] + slot, layers) * sizes["y"] + side
        start = pl.multiple_of(place * unit, unit)
        if kind >= 2:
            source = down_hbm.at[pl.ds(start, unit), pl.ds((kind - 2) * sub, sub)]
        else:
            source = (value_hbm, gate_hbm)[kind].at[:, pl.ds(start, unit)]
        return core * per + place, source

    def weight_copy(kind, slot):
        shift = (slot // layers + 1) % sizes["y"]
        chip, source = cut_of(kind, slot, mine["y"])
        from_y = lax.rem(mine["y"] + sizes["y"] - shift, sizes["y"])
        origin = mine["z"] * sizes["y"] + from_y
        keeper = lax.rem(origin, cores)
        if shift:
            source = (held_down.at[slot, kind - 2] if kind >= 2 else held_up.at[slot, kind])
        stays = (chip == sp) & (keeper == core)
        target = block_view(kind, origin)
        device = (chip, mine["x"] * cores + keeper)

        def here():
            return pltpu.make_async_copy(source, target, w_recv.at[kind, origin // cores])

        def away():
            return remote(source, target, w_send.at[kind, slot], w_recv.at[kind, origin // cores], device)

        return stays, here, away

    def hold_copy(kind, slot):
        side = lax.rem(mine["y"] + slot // layers + 1, sizes["y"])
        _, source = cut_of(kind, slot, side)
        held = held_down.at[slot, kind - 2] if kind >= 2 else held_up.at[slot, kind]
        device = (mine["z"] * sizes["y"] + side, tp)
        return remote(source, held, hold_send.at[kind, slot], hold_recv.at[kind, slot], device)

    def hand_over(kinds, slots):
        for slot in slots:
            for kind in kinds:
                hold_copy(kind, slot).start()

    def send_weights(kinds, slots):
        for slot in slots:
            for kind in kinds:
                if slot in across:
                    hold_copy(kind, slot).wait_recv()
                stays, here, away = weight_copy(kind, slot)
                pl.when(stays)(lambda: here().start())
                pl.when(jnp.logical_not(stays))(lambda: away().start())

    def finish_sends():
        for slot in range(per):
            for kind in range(2 + halves):
                if slot in across:
                    hold_copy(kind, slot).wait_send()
                stays, _, away = weight_copy(kind, slot)
                pl.when(jnp.logical_not(stays))(lambda: away().wait_send())

    def passed_on(kinds, side, index):
        source = side + cores * index
        if kinds[0] >= 2:
            view = block_view(kinds[0], source)
        else:
            view = up_w.at[pl.ds(pl.multiple_of(source * depth, depth), depth), :]
        at = max(kinds[0] - 1, 0)
        return remote(view, view, f_send.at[at, index], f_recv.at[at, index], partner)

    def forward_weights(kinds):
        started = []
        for index in range(per):
            for kind in kinds:
                view = block_view(kind, core + cores * index)
                remote(view, view, w_send.at[kind, 0], w_recv.at[kind, index], partner).wait_recv()
            copy = passed_on(kinds, core, index)
            copy.start()
            started.append(copy)
        return started

    def forwarded(kinds, started):
        for copy in started:
            copy.wait_send()
        for index in range(per):
            passed_on(kinds, lax.rem(core + 1, cores), index).wait_recv()

    hand_over((0,), across[:1])
    send_weights((0,), straight[:1])

    early_copies = []

    sends_at = {"gain": 0, "total": tp_count, "carry": tp_count + count}
    sends_at["y"] = sends_at["edge"] = sends_at["carry"]
    lands_at = dict(sends_at)
    lands_at["y"] = lands_at["carry"] + count
    lands_at["edge"] = lands_at["y"] + tp_count

    def small(source, target, kind, index, device):
        send = small_send.at[sends_at[kind] + index - 1]
        return remote(source, target, send, small_recv.at[lands_at[kind] + index - 1], device)

    for offset in range(1, tp_count):
        peer = (sp, lax.rem(tp + offset, tp_count))
        copy = small(gain_ref, gain_all.at[tp], "gain", offset, peer)
        copy.start()
        early_copies.append(copy)
    gain_all[tp] = gain_ref[...]

    owns_taps = core == sp // per
    taps_start = pl.ds(pl.multiple_of(lax.rem(sp, per) * unit, unit), unit)
    taps_copies = []
    for kind, source in enumerate((value_taps_ref, gate_taps_ref)):
        view = source.at[:, taps_start]
        keep = pltpu.make_async_copy(view, taps.at[kind], taps_sem.at[3 * kind])
        send = remote(
            view, taps.at[kind], taps_sem.at[3 * kind + 1], taps_sem.at[3 * kind + 2], partner
        )
        taps_copies.append((keep, send))

    @pl.when(owns_taps)
    def _():
        for keep, send in taps_copies:
            keep.start()
            send.start()

    pick_group = lax.broadcasted_iota(jnp.int32, (groups, lanes), 0)
    pick_side = lax.broadcasted_iota(jnp.int32, (groups, lanes), 1) // states
    pick_odd = (lax.rem(pick_group, 2) == pick_side).astype(jnp.bfloat16)
    own_pair = lax.broadcasted_iota(
        jnp.int32, (pairs, groups), 1
    ) // 2 == lax.broadcasted_iota(jnp.int32, (pairs, groups), 0)

    def over_lanes(row):
        left = jnp.where(own_pair, jnp.broadcast_to(row, (pairs, groups)), 0.0)
        found = jnp.zeros((pairs, lanes), jnp.float32)
        for _ in range(3):
            rounded = left.astype(jnp.bfloat16)
            found = found + jnp.dot(rounded, pick_odd, preferred_element_type=jnp.float32)
            left = left - rounded.astype(jnp.float32)
        return found

    number = lax.rem(lax.broadcasted_iota(jnp.int32, (8, lanes), 1), states).astype(jnp.float32)
    near = lax.broadcasted_iota(jnp.int32, (8, lanes), 0).astype(jnp.float32)
    for k in range(2):
        step_size = step_ref[k : k + 1, :]
        log_decay = -0.5 * step_size - jnp.transpose(damping_ref[k])
        rows_at = pl.ds(k * pairs, pairs)
        totals[rows_at, :] = over_lanes(jnp.exp(jnp.sum(log_decay, axis=0, keepdims=True)))
        left = jnp.exp(log_decay)
        for level in range(3):
            rounded = left.astype(jnp.bfloat16)
            decay_parts[k, :, level * groups : (level + 1) * groups] = rounded
            left = left - rounded.astype(jnp.float32)
    total_copies = []
    for offset in range(1, count):
        peer = (lax.rem(sp + offset, count), tp)
        copy = small(totals, totals_all.at[sp], "total", offset, peer)
        copy.start()
        total_copies.append(copy)
    totals_all[sp] = totals[...]
    for k in range(2):
        step_size = step_ref[k : k + 1, :]
        rows_at = pl.ds(k * pairs, pairs)
        wide_step = over_lanes(step_size)
        turn_ref[2, rows_at, :] = over_lanes(drive_scale(step_size))
        cos, sin = turned(turns_of(wide_step, number * span))
        turn_ref[0, rows_at, :] = cos
        turn_ref[1, rows_at, :] = sin
        reach = near + 1.0 if k == 0 else 8.0 - near
        for pair in range(pairs):
            cos, sin = turned(turns_of(wide_step[pair : pair + 1], number * reach))
            tab_ref[k * pairs + pair, 0] = cos
            tab_ref[k * pairs + pair, 1] = sin

    x_t[...] = jnp.transpose(x_ref[...].astype(jnp.float32)).astype(jnp.bfloat16)
    row_in_tile = lax.broadcasted_iota(jnp.int32, (1, 8, lanes), 1)
    pick_row = lax.rem(lax.broadcasted_iota(jnp.int32, (3 * groups, lanes), 0), groups)
    pick_lane = lax.broadcasted_iota(jnp.int32, (3 * groups, lanes), 1) // (lanes // 2)

    def both_groups(ref, pair):
        blocks_of = []
        empty = jnp.zeros((head, states), jnp.float32)
        for k in range(2):
            for kind in range(2):
                first = ref[k, kind, 2 * pair].astype(jnp.float32)
                second = ref[k, kind, 2 * pair + 1].astype(jnp.float32)
                upper = jnp.concatenate((first, empty), axis=1)
                lower = jnp.concatenate((empty, second), axis=1)
                blocks_of.append(jnp.concatenate((upper, lower), axis=0))
        return jnp.concatenate(blocks_of, axis=1)

    def chain(k, at, start_real, start_imag):
        real, imag = start_real, start_imag
        found = [None] * tiles
        for tile in range(tiles) if k == 0 else range(tiles - 1, -1, -1):
            place = pl.ds(tile * 8, 8)
            cos, sin = carried[at, 0, place, :], carried[at, 1, place, :]
            full_real = local[at, 0, place, :] + (cos * real - sin * imag)
            full_imag = local[at, 1, place, :] + (cos * imag + sin * real)
            found[tile] = (full_real, full_imag)
            edge = slice(7, 8) if k == 0 else slice(0, 1)
            real = jnp.broadcast_to(full_real[edge], (8, lanes))
            imag = jnp.broadcast_to(full_imag[edge], (8, lanes))
        return found, real, imag

    def first_pass(pair, _):
        inputs = x_t[pl.ds(pl.multiple_of(pair * heads, heads), heads), :]
        driven = lax.dot_general(
            inputs,
            both_groups(in_ref, pair).astype(jnp.bfloat16),
            (((0,), (0,)), ((), ())),
            preferred_element_type=jnp.float32,
        )
        for k in range(2):
            at = k * pairs + pair
            pick = (pick_row == 2 * pair + pick_lane).astype(jnp.bfloat16)
            cover = jnp.dot(decay_parts[k], pick, preferred_element_type=jnp.float32)
            cover = cover.reshape(tiles, 8, lanes)
            base = 2 * k * lanes
            scale = turn_ref[2, pl.ds(at, 1), :]
            real = (driven[:, base : base + lanes] * scale).reshape(tiles, 8, lanes)
            imag = (driven[:, base + lanes : base + 2 * lanes] * scale).reshape(tiles, 8, lanes)
            for reach in (1, 2, 4):
                row = reach - 1 if k == 0 else 8 - reach
                shift = reach if k == 0 else 8 - reach
                valid = row_in_tile >= reach if k == 0 else row_in_tile < 8 - reach
                cos = tab_ref[at, 0, row : row + 1, :].reshape(1, 1, lanes)
                sin = tab_ref[at, 1, row : row + 1, :].reshape(1, 1, lanes)
                moved_real = pltpu.roll(real, shift, 1)
                moved_imag = pltpu.roll(imag, shift, 1)
                decay = jnp.where(valid, cover, 0.0)
                real = real + decay * (cos * moved_real - sin * moved_imag)
                imag = imag + decay * (cos * moved_imag + sin * moved_real)
                cover = cover * jnp.where(valid, pltpu.roll(cover, shift, 1), 1.0)
            local[at, 0] = real.reshape(span, lanes)
            local[at, 1] = imag.reshape(span, lanes)
            carried[at, 0] = (cover * tab_ref[at, 0].reshape(1, 8, lanes)).reshape(span, lanes)
            carried[at, 1] = (cover * tab_ref[at, 1].reshape(1, 8, lanes)).reshape(span, lanes)
        for k in range(2):
            at = k * pairs + pair
            none = jnp.zeros((8, lanes), jnp.float32)
            real, imag = chain(k, at, none, none)[1:]
            ends[pl.ds(at, 1), :] = real[0:1]
            ends[pl.ds(2 * pairs + at, 1), :] = imag[0:1]
        return _

    lax.fori_loop(0, pairs, first_pass, 0)

    packet[...] = ends[...].astype(jnp.bfloat16)
    packets[sp] = packet[...]
    carry_copies = []
    for offset in range(1, count):
        peer = (lax.rem(sp + offset, count), tp)
        copy = small(packet, packets.at[sp], "carry", offset, peer)
        copy.start()
        carry_copies.append(copy)
    for copy in total_copies + carry_copies:
        copy.wait()
    hand_over((1,), across[:1])
    hand_over((0, 1), across[1:])
    send_weights((1,), straight[:1])
    send_weights((0,), straight[1:])

    for k in range(2):
        at = pl.ds(k * pairs, pairs)
        cos, sin = turn_ref[0, at, :], turn_ref[1, at, :]
        real = jnp.zeros((pairs, lanes), jnp.float32)
        imag = real
        for index in range(count) if k == 0 else range(count - 1, -1, -1):
            total = totals_all[index, at, :]
            end = packets[index].astype(jnp.float32)
            end_real = end[k * pairs : (k + 1) * pairs]
            end_imag = end[(2 + k) * pairs : (3 + k) * pairs]
            turned_real = cos * real - sin * imag
            turned_imag = cos * imag + sin * real
            before = (index < sp) if k == 0 else (index > sp)
            real = jnp.where(before, end_real + total * turned_real, real)
            imag = jnp.where(before, end_imag + total * turned_imag, imag)
        carry[0, at, :] = real
        carry[1, at, :] = imag

    gains = skip_ref[...] * x_ref[...].astype(jnp.float32)
    for pair in range(pairs):
        parts = []
        for k in range(2):
            at = k * pairs + pair
            real = jnp.broadcast_to(carry[0, at : at + 1, :], (8, lanes))
            imag = jnp.broadcast_to(carry[1, at : at + 1, :], (8, lanes))
            found, _, _ = chain(k, at, real, imag)
            parts.append(jnp.concatenate([item[0] for item in found], axis=0))
            parts.append(jnp.concatenate([item[1] for item in found], axis=0))
        state = jnp.concatenate(parts, axis=1)
        state_high = state.astype(jnp.bfloat16)
        state_low = (state - state_high.astype(jnp.float32)).astype(jnp.bfloat16)
        sign = jnp.concatenate([jnp.full((1, lanes), v, jnp.float32) for v in (1, -1, 1, -1)], axis=1)
        out_map = both_groups(readout_ref, pair) * sign
        map_high = out_map.astype(jnp.bfloat16)
        map_low = (out_map - map_high.astype(jnp.float32)).astype(jnp.bfloat16)

        def apply(left, right):
            return lax.dot_general(
                left, right, (((1,), (1,)), ((), ())), preferred_element_type=jnp.float32
            )

        both = apply(state_high, jnp.concatenate((map_high, map_low), axis=0))
        mixed = both[:, :heads] + both[:, heads:] + apply(state_low, map_high)
        columns = slice(pair * heads, (pair + 1) * heads)
        y_all[:, columns] = (mixed + gains[:, columns]).astype(jnp.bfloat16)
    y_copies = []
    for offset in range(1, tp_count):
        peer = lax.rem(tp + offset, tp_count)
        part_rows = y_all.at[pl.ds(pl.multiple_of(peer * rows, rows), rows), :]
        copy = small(part_rows, y_land.at[tp], "y", offset, (sp, peer))
        copy.start()
        y_copies.append(copy)
    y_land[tp] = y_all[pl.ds(pl.multiple_of(tp * rows, rows), rows), :]
    for copy in early_copies + y_copies:
        copy.wait()
    out_copy.wait()

    mixed = jnp.concatenate([y_land[peer] for peer in range(tp_count)], axis=1)
    mixed = mixed.astype(jnp.float32)
    gain = jnp.concatenate([gain_all[peer] for peer in range(tp_count)], axis=1)
    inverse = lax.rsqrt(jnp.mean(mixed * mixed, axis=1, keepdims=True) + norm_eps)
    normed_mix = (mixed * inverse * gain).astype(jnp.bfloat16)
    square = jnp.zeros((rows, 1), jnp.float32)
    tile = 512
    for start in range(0, width, tile):
        columns = pl.ds(start, tile)
        mixed_rows = jnp.dot(normed_mix, out_w[:, columns], preferred_element_type=jnp.float32)
        summed = (residual_ref[:, columns].astype(jnp.float32) + mixed_rows).astype(jnp.bfloat16)
        state_rows[:, columns] = summed
        wide = summed.astype(jnp.float32)
        square = square + jnp.sum(wide * wide, axis=1, keepdims=True)
    scale_rows = lax.rsqrt(square / width + norm_eps)
    normed = state_rows[...].astype(jnp.float32) * scale_rows * channel_ref[...]
    rows_all[mine["z"], mine["y"], mine["x"]] = normed.astype(jnp.bfloat16)

    deep = sizes["z"] // 2
    base = mine["z"] // deep * deep
    other = deep - base
    relays = mine["z"] == deep - 1 + base // deep
    far_end = deep - base // deep

    def plane(z):
        return z * sizes["y"] + mine["y"], tp

    def line_copy(piece, source, target, at):
        columns = pl.ds(piece * piece_width, piece_width)
        view = rows_all.at[source, mine["y"], mine["x"], :, columns]
        return remote(
            view, view, line_send.at[piece, at], line_recv.at[piece, source], plane(target)
        )

    def line_start(piece):
        line_copy(piece, mine["z"], far_end, 0).start()
        for offset in range(1, deep):
            line_copy(piece, mine["z"], base + lax.rem(mine["z"] + offset, deep), offset).start()

    def line_relay(piece, action):
        for index in range(deep):
            for offset in range(1, deep):
                at = deep + index * (deep - 1) + offset - 1
                target = base + lax.rem(mine["z"] + offset, deep)
                copy = line_copy(piece, other + index, target, at)
                copy.start() if action == "start" else copy.wait_send()

    def line_finish(piece):
        for index in range(deep):
            line_copy(piece, other + index, far_end, 0).wait_recv()
        pl.when(relays)(lambda: line_relay(piece, "start"))
        for offset in range(1, deep):
            source = base + lax.rem(mine["z"] + offset, deep)
            line_copy(piece, source, far_end, 0).wait_recv()

    def line_sent(piece):
        for at in range(deep):
            line_copy(piece, mine["z"], far_end, at).wait_send()
        pl.when(relays)(lambda: line_relay(piece, "sent"))

    for piece in range(pieces):
        line_start(piece)

    send_weights((1,), straight[1:])

    slot = 0
    sums_at = pieces * (sizes["y"] + sizes["x"] - 2)
    pending = [[] for _ in range(pieces)]
    steps = [(piece + 3 * stage, stage, piece) for stage in (1, 2) for piece in range(pieces)]
    for _, stage, piece in sorted(steps):
        if stage == 1:
            line_finish(piece)
        axis = gather_paths[piece][stage]
        done = gather_paths[piece][:stage]
        for copy in pending[piece]:
            copy.wait()
        pending[piece] = []
        index = tuple(slice(None) if name in done else mine[name] for name in chip_axes)
        block = rows_all.at[index + (slice(None), pl.ds(piece * piece_width, piece_width))]
        for offset in range(1, sizes[axis]):
            _, device = neighbour(axis, offset)
            copy = remote(block, block, hop_send.at[slot], hop_recv.at[slot], device)
            copy.start()
            pending[piece].append(copy)
            slot += 1
        if stage == 1 and piece == pieces - 1:
            send_weights((0, 1), across)
    for kind in range(2, 2 + halves):
        hand_over((kind,), across)
        send_weights((kind,), straight)
    up_started = forward_weights((0, 1))
    for piece in range(pieces):
        for copy in pending[piece]:
            copy.wait()
    for piece in range(pieces):
        line_sent(piece)
    forwarded((0, 1), up_started)

    @pl.when(core == 0)
    def _():
        up_rows[1, pl.ds(0, 8), :] = jnp.zeros((8, 2 * unit), jnp.float32)

    @pl.when(core == cores - 1)
    def _():
        up_rows[blocks, pl.ds(rows + 8, 8), :] = jnp.zeros((8, 2 * unit), jnp.float32)

    chunk = 256

    def project(n, _):
        columns = pl.ds(pl.multiple_of(n * chunk, chunk), chunk)
        block = rows_all[...].reshape(blocks * rows, width)
        up = jnp.dot(block, up_w[:, columns], preferred_element_type=jnp.float32)
        up = up.astype(jnp.bfloat16).astype(jnp.float32)
        up_rows[pl.ds(1, blocks), pl.ds(8, rows), columns] = up.reshape(blocks, rows, chunk)
        return _

    lax.fori_loop(0, 2 * unit // chunk, project, 0)

    edges = []
    for kind, (take, land, first) in enumerate(((rows, 0, 1 + core), (8, rows + 8, core))):
        edge = up_rows.at[pl.ds(1, blocks), pl.ds(take, 8), :]
        beyond = up_rows.at[pl.ds(first, blocks), pl.ds(land, 8), :]
        copy = small(edge, beyond, "edge", kind + 1, partner)
        copy.start()
        edges.append(copy)
    for kind in range(2, 2 + halves):
        send_weights((kind,), across)

    @pl.when(owns_taps)
    def _():
        for keep, send in taps_copies:
            keep.wait()
            send.wait_send()

    @pl.when(jnp.logical_not(owns_taps))
    def _():
        for _, send in taps_copies:
            send.wait_recv()

    for copy in edges:
        copy.wait()

    def mix(b, _):
        window = up_rows[b + 1]

        def conv(kind, columns):
            return (
                taps[kind, 0:1, :] * window[7 : rows + 7, columns]
                + taps[kind, 1:2, :] * window[8 : rows + 8, columns]
                + taps[kind, 2:3, :] * window[9 : rows + 9, columns]
            )

        value = conv(0, slice(0, unit))
        gate = conv(1, slice(unit, 2 * unit))
        hidden = value * (gate / (1.0 + jnp.exp(-gate)))
        hidden_rows[pl.ds(pl.multiple_of(b * rows, rows), rows), :] = hidden.astype(jnp.bfloat16)
        return _

    lax.fori_loop(0, blocks, mix, 0)

    sum_width = width // sums_in
    per_half = sums_in // halves

    def start_sum(piece, stage, slot):
        axis = sum_paths[piece][stage]
        done = sum_paths[piece][:stage]
        started = []
        for offset in range(1, sizes[axis]):
            place, device = neighbour(axis, offset)
            index = tuple(
                place if name == axis else mine[name] if name in done else slice(None)
                for name in chip_axes
            )
            copy = remote(
                partial.at[index + (slice(None), pl.ds(piece * sum_width, sum_width))],
                landing[piece * 3 + stage].at[offset - 1],
                hop_send.at[slot],
                hop_recv.at[slot],
                device,
            )
            copy.start()
            started.append(copy)
            slot += 1
        return started, slot

    def add_landed(piece, stage):
        axis = sum_paths[piece][stage]
        done = sum_paths[piece][: stage + 1]
        land = landing[piece * 3 + stage]
        columns = pl.ds(piece * sum_width, sum_width)
        free = [name for name in chip_axes if name not in done]

        def add(step, _):
            index, inner = [], ()
            for name in chip_axes:
                if name in done:
                    index.append(mine[name])
                elif name == free[0]:
                    index.append(step)
                    inner = (step,)
                else:
                    index.append(slice(None))
            index = tuple(index) + (slice(None), columns)
            value = partial[index].astype(jnp.float32)
            for offset in range(1, sizes[axis]):
                value = value + land[(offset - 1,) + inner].astype(jnp.float32)
            if free:
                partial[index] = value.astype(jnp.bfloat16)
            else:
                for step_at in range(sum_width // sub):
                    place = piece % per_half * sum_width // sub + step_at
                    real = pl.ds(place * part + piece // per_half * sub, sub)
                    added = value[:, step_at * sub : (step_at + 1) * sub]
                    out_ref[:, real] = (
                        state_rows[:, real].astype(jnp.float32) + added
                    ).astype(jnp.bfloat16)
            return _

        if free:
            lax.fori_loop(0, sizes[free[0]], add, 0)
        else:
            add(0, 0)

    slot = sums_at
    waiting = {}

    def advance(pair, stage, slot):
        for piece in range(2 * pair, 2 * pair + 2):
            if stage == 0:
                columns = pl.ds(piece % per_half * sum_width, sum_width)
                sums = jnp.dot(
                    hidden_rows[...],
                    down_w[piece // per_half, :, columns],
                    preferred_element_type=jnp.float32,
                )
                shape = partial.shape[:3] + (rows, sum_width)
                partial[:, :, :, :, pl.ds(piece * sum_width, sum_width)] = sums.astype(
                    jnp.bfloat16
                ).reshape(shape)
            else:
                for copy in waiting[piece]:
                    copy.wait()
                add_landed(piece, stage - 1)
            if stage < 3:
                waiting[piece], slot = start_sum(piece, stage, slot)
        return slot

    pair_count = sums_in // 2
    plan = sorted(
        (2 * pair + 3 * stage, stage, pair) for pair in range(pair_count) for stage in range(4)
    )
    down_started = forward_weights((2,))
    ready = 0
    for _, stage, pair in plan:
        group = 2 * pair // per_half
        if stage == 0 and 2 * pair % per_half == 0:
            forwarded((2 + group,), down_started)
            ready = group
        slot = advance(pair, stage, slot)
        if stage == 0 and ready + 1 < halves and (2 * pair + 2) % per_half == 0:
            down_started = forward_weights((3 + ready,))
    finish_sends()


def whole_layer(sizes, arrays, weights, unit):
    x, time_step, _, in_map, _, _, gain, value_taps, _, residual, _ = arrays
    out_weight, value_weight, gate_weight, down_weight = weights
    span, channels = x.shape
    groups, lanes = time_step.shape[1], 2 * in_map.shape[4]
    chains = groups
    rows, width = residual.shape
    pieces, sums_in = len(gather_paths), len(sum_paths)
    count, tp_count = sizes["z"] * sizes["y"], sizes["x"] * sizes["c"]
    grid = tuple(sizes[name] for name in chip_axes)
    blocks = math.prod(grid)
    per = count // sizes["c"]
    landing = []
    for order in sum_paths:
        for stage in range(3):
            axis = order[stage]
            left = tuple(sizes[name] for name in chip_axes if name not in order[: stage + 1])
            landing.append(
                pltpu.VMEM((max(sizes[axis] - 1, 1),) + left + (rows, width // sums_in), jnp.bfloat16)
            )
    gather_hops = pieces * (sizes["y"] + sizes["x"] - 2)
    sum_hops = sums_in * sum(sizes[name] - 1 for name in chip_axes)
    deep = sizes["z"] // 2
    aside = max(per - per // sizes["y"], 1)
    vmem = pl.BlockSpec(memory_space=pltpu.VMEM)
    far = pl.BlockSpec(memory_space=pl.ANY)
    dma = pltpu.SemaphoreType.DMA
    f32, bf16 = jnp.float32, jnp.bfloat16
    return pl.pallas_call(
        lambda *refs: layer_kernel(sizes, *refs),
        name="whole_layer",
        out_shape=jax.ShapeDtypeStruct((rows, width), bf16),
        in_specs=[vmem] * 11 + [far] * 4,
        out_specs=vmem,
        scratch_shapes=[
            pltpu.VMEM((channels, span), bf16),
            pltpu.VMEM((2, span, 3 * groups), bf16),
            pltpu.VMEM((chains, 2, span, lanes), f32),
            pltpu.VMEM((chains, 2, span, lanes), f32),
            pltpu.VMEM((chains, 2, 8, lanes), f32),
            pltpu.VMEM((3, chains, lanes), f32),
            pltpu.VMEM((chains, lanes), f32),
            pltpu.VMEM((count, chains, lanes), f32),
            pltpu.VMEM((2 * chains, lanes), f32),
            pltpu.VMEM((2 * chains, lanes), bf16),
            pltpu.VMEM((count, 2 * chains, lanes), bf16),
            pltpu.VMEM((2, chains, lanes), f32),
            pltpu.VMEM((span, channels), bf16),
            pltpu.VMEM((tp_count, rows, channels), bf16),
            pltpu.VMEM((tp_count,) + gain.shape, f32),
            pltpu.VMEM(out_weight.shape, bf16),
            pltpu.VMEM((rows, width), bf16),
            pltpu.VMEM((2, value_taps.shape[0], unit), f32),
            pltpu.VMEM((width, 2 * unit), bf16),
            pltpu.VMEM((halves, unit, width // halves), bf16),
            pltpu.VMEM((aside, 2, width // count, unit), bf16),
            pltpu.VMEM((aside, halves, unit, width // count // halves), bf16),
            pltpu.VMEM(grid + (rows, width), bf16),
            pltpu.VMEM((blocks + 2, rows + 16, 2 * unit), f32),
            pltpu.VMEM((blocks * rows, unit), bf16),
            pltpu.VMEM(grid + (rows, width), bf16),
            *landing,
            dma((1,)),
            dma((tp_count + 2 * count + 2,)),
            dma((2 * tp_count + 2 * count + 2,)),
            dma((6,)),
            dma((gather_hops + sum_hops,)),
            dma((gather_hops + sum_hops,)),
            dma((pieces, deep * deep)),
            dma((pieces, sizes["z"])),
            dma((2 + halves, aside)),
            dma((2 + halves, aside)),
            dma((2 + halves, per)),
            dma((2 + halves, per)),
            dma((1 + halves, per)),
            dma((1 + halves, per)),
        ],
        compiler_params=pltpu.CompilerParams(
            collective_id=2, has_side_effects=True, vmem_limit_bytes=63 * 1024 * 1024
        ),
    )(*arrays, *weights)


def mesh_sizes(sp_count, tp_count):
    cores = 2
    across = tp_count // cores
    deep = math.gcd(across, sp_count)
    return {"z": sp_count // deep, "y": deep, "x": across, "c": cores}


def tile_units(sizes, x_shape, in_shape, value_shape, down_shape, residual_shape):
    count = sizes["z"] * sizes["y"]
    unit = value_shape[1] * sizes["c"] // count
    rows, width = residual_shape
    span, states, head = x_shape[0], in_shape[3], in_shape[4]
    fits = (
        sizes["z"] % 2 == 0
        and sizes["z"] % sizes["c"] == 0
        and unit % 128 == 0
        and 2 * unit % 256 == 0
        and value_shape[0] % 16 == 0
        and down_shape[1] % (128 * halves) == 0
        and width // len(sum_paths) % (down_shape[1] // halves) == 0
        and width % 512 == 0
        and rows % 16 == 0
        and span % 128 == 0
        and 2 * states == 128
        and in_shape[2] % 16 == 0
        and width % (256 * len(gather_paths)) == 0
        and head % 16 == 0
        and x_shape[1] % 128 == 0
    )
    return unit if fits else 0


def one_kernel(sizes, unit, args):
    (
        mixer_input,
        time_step,
        damping,
        input_map,
        readout,
        skip_gain,
        out_gain,
        out_weight,
        residual,
        channel_gain,
        value_weight,
        gate_weight,
        value_taps,
        gate_taps,
        down_weight,
    ) = args
    arrays = (
        mixer_input,
        time_step,
        damping.swapaxes(1, 2),
        input_map.swapaxes(3, 4),
        readout,
        skip_gain.reshape(1, -1),
        out_gain.reshape(1, -1),
        value_taps,
        gate_taps,
        residual,
        channel_gain.reshape(1, -1),
    )
    return whole_layer(
        sizes, arrays, (out_weight, value_weight, gate_weight, down_weight), unit
    )


def body(
    mixer_input,
    time_step,
    damping,
    input_map,
    readout,
    skip_gain,
    out_gain,
    out_weight,
    residual,
    channel_gain,
    value_weight,
    gate_weight,
    value_taps,
    gate_taps,
    down_weight,
):
    count, mine = lax.axis_size("sp"), lax.axis_index("sp")
    sizes = mesh_sizes(count, lax.axis_size("tp"))
    unit = tile_units(
        sizes,
        mixer_input.shape,
        input_map.shape,
        value_weight.shape,
        down_weight.shape,
        residual.shape,
    )
    if unit:
        args = (mixer_input, time_step, damping, input_map, readout, skip_gain, out_gain)
        args += (out_weight, residual, channel_gain, value_weight, gate_weight)
        return one_kernel(sizes, unit, args + (value_taps, gate_taps, down_weight))
    depth, hidden_width = value_weight.shape
    part = hidden_width // count
    up_send = jnp.concatenate(
        (
            value_weight.reshape(depth, count, part).swapaxes(0, 1),
            gate_weight.reshape(depth, count, part).swapaxes(0, 1),
        ),
        axis=2,
    )
    down_send = down_weight.reshape(count, part, down_weight.shape[1])
    mixed_y = mixer(mixer_input, time_step, damping, input_map, readout, skip_gain)
    tp_count = lax.axis_size("tp")
    mixed_y = mixed_y.reshape(tp_count, -1, out_gain.shape[0])
    gain_row = jnp.broadcast_to(out_gain, (tp_count, 1, out_gain.shape[0]))
    mixed_y = jnp.concatenate((mixed_y, gain_row), axis=1)
    mixed_y = lax.all_to_all(mixed_y, "tp", split_axis=0, concat_axis=0, tiled=True)
    mixed_y = mixed_y.swapaxes(0, 1).reshape(mixed_y.shape[1], -1)
    mixed_y, gain = mixed_y[:-1], mixed_y[-1]
    inverse = lax.rsqrt(jnp.mean(mixed_y * mixed_y, axis=1, keepdims=True) + norm_eps)
    normed_mix = (mixed_y * inverse * gain[None, :]).astype(jnp.bfloat16)
    mixed_rows = jnp.dot(normed_mix, out_weight, preferred_element_type=jnp.float32)
    hidden_state = (residual.astype(jnp.float32) + mixed_rows).astype(jnp.bfloat16)
    state_wide = hidden_state.astype(jnp.float32)
    scale_rows = lax.rsqrt(jnp.mean(state_wide * state_wide, axis=1, keepdims=True) + norm_eps)
    normed = (state_wide * scale_rows * channel_gain[None, :]).astype(jnp.bfloat16)
    taps = jnp.concatenate(
        (
            lax.dynamic_slice_in_dim(value_taps, mine * part, part, axis=1),
            lax.dynamic_slice_in_dim(gate_taps, mine * part, part, axis=1),
        ),
        axis=1,
    )
    return channel_mixer(normed, hidden_state, up_send, down_send, taps, count, tp_count)


def solution(mesh):
    in_specs = (
        P("sp", "tp"),
        P(None, "tp"),
        P(None, "sp", "tp"),
        P(None, None, "tp", None, None),
        P(None, None, "tp", None, None),
        P("tp"),
        P("tp"),
        P(),
        P(("sp", "tp"), None),
        P(),
        P("sp", "tp"),
        P("sp", "tp"),
        P(None, "tp"),
        P(None, "tp"),
        P("tp", "sp"),
    )
    out_specs = P(("sp", "tp"), None)
    return jax.shard_map(body, mesh=mesh, in_specs=in_specs, out_specs=out_specs, check_vma=False)
```
